32 devices in a mesh: grp: 2 (over x), sp: 8 (over z, y), tp: 2 (over core).
Axes of the slice: x: 2, y: 2, z: 4, core: 2. Of those that a mesh axis runs over, the one named last changes fastest.
Arguments:
- tokens: bfloat16 [8192, 2048], P(('grp', 'sp', 'tp')), parts along dimension 0, may hold values from -64 to 64
- w_query: bfloat16 [2048, 1024], P(None, 'tp'), may hold values from -0.125 to 0.125
- w_key: bfloat16 [2048, 1024], P(None, 'tp'), may hold values from -0.125 to 0.125
- w_value: bfloat16 [2048, 1024], P(None, 'tp'), may hold values from -0.25 to 0.25
- w_out: bfloat16 [1024, 2048], P('tp'), may hold values from -0.1875 to 0.1875
Outputs:
- mixed: bfloat16 [8192, 2048], P(('grp', 'sp', 'tp')), parts along dimension 0
- log_sums: float32 [16, 8192], P('tp', ('grp', 'sp')), parts along dimension 1
The draws below stay inside these ranges and needn't reach their ends.
There are 2 independent parts, one for each index of `grp`. The reference program is written for one: setup_inputs(seed, part) draws one part's arguments, and reference() takes and returns one part's arrays. A program takes and returns all parts, laid end to end along the dimension named above; an argument that names none is the same for every part. Nothing has to cross between parts.
All inputs are finite; a program needn't handle non-finite values.
Results may differ from the reference program's by a relative error of at most 0.013.
The reference program's roundings to bfloat16 on the way count: a program that leaves them out, or rounds other values in their place, can miss the bound.
Values may be sent and summed in bfloat16 or wider, within the bound.
A program may use at most 128 MiB of HBM per device.

```python
import math
import jax
import jax.numpy as jnp
from jax import lax

D = 2048
HEADS = 16
HEAD_DIM = 64
WINDOW_KEY_STEPS = 128
MIDDLE_DILATION = 4
FAR_DILATION = 16
TOK_DEV = 512
TOKENS = 4096
REACH = 2048
N_SP = 8
N_TP = 2


def draw_tokens(key, part):
    base = jnp.clip(jax.random.normal(jax.random.fold_in(key, 11), (TOKENS, D), jnp.float32), -4.0, 4.0)
    return base.astype(jnp.bfloat16)


def block_levels(own_key, dims, split, least, largest):
    loudness = 1.0
    for position, shards_of in split:
        steps = jax.random.uniform(jax.random.fold_in(jax.random.fold_in(own_key, 6), position), (shards_of,), jnp.float32, least / len(split), largest / len(split))
        loudness = loudness * jnp.repeat(jnp.exp(steps), dims[position] // shards_of).reshape((-1,) + (1,) * (len(dims) - 1 - position))
    return loudness


def bell_draw(key, dims, scale, bound, split=(), kind=jnp.bfloat16):
    result = scale * jax.random.normal(key, dims, jnp.float32)
    if split:
        result = result * block_levels(key, dims, split, -0.22, 0.18)
    return jnp.clip(result, -bound, bound).astype(kind)


def setup_inputs(seed: int = 0, part: int = 0) -> dict:
    key_list = jax.random.split(jax.random.key(seed), 6)
    part_splits = jax.random.split(jax.random.fold_in(key_list[5], part), 6)
    tokens = draw_tokens(jax.random.fold_in(jax.random.fold_in(key_list[5], part), 71), part)
    w_query = bell_draw(key_list[1], (D, HEADS * HEAD_DIM), D ** -0.5, 0.125, ((1, 2),))
    w_key = bell_draw(key_list[2], (D, HEADS * HEAD_DIM), D ** -0.5, 0.125, ((1, 2),))
    w_value = bell_draw(key_list[3], (D, HEADS * HEAD_DIM), (D // 4) ** -0.5, 0.25, ((1, 2),))
    w_out = bell_draw(key_list[4], (HEADS * HEAD_DIM, D), (HEADS * HEAD_DIM) ** -0.5, 0.1875, ((0, 2),))
    return dict(tokens=tokens, w_query=w_query, w_key=w_key, w_value=w_value, w_out=w_out)


ALIBI_EXP = 16.0


def dilated_attention(query_rows, key_value_rows, dilation, window_steps, head_slopes, first_position):
    length, heads, depth = query_rows.shape
    total_rows = key_value_rows.shape[0]
    strided = length // dilation
    block_rows = math.gcd(strided, 128)
    num_blocks = strided // block_rows
    behind = (total_rows - length) // dilation
    grouped = query_rows.reshape(num_blocks, block_rows, dilation, heads, depth)
    columns = key_value_rows.reshape(total_rows // dilation, dilation, 2, heads, depth)
    spans = jnp.stack([columns[behind + index * block_rows - window_steps: behind + (index + 1) * block_rows]
                       for index in range(num_blocks)])
    scores = jnp.einsum("bqrhe,bkrhe->brhqk", grouped.astype(jnp.float32),
                        spans[:, :, :, 0].astype(jnp.float32)) * depth ** -0.5
    row_pos = jnp.arange(block_rows, dtype=jnp.int32)[:, None]
    key_pos = jnp.arange(window_steps + block_rows, dtype=jnp.int32)[None, :]
    distance = window_steps + row_pos - key_pos
    inside = (distance >= 0) & (distance <= window_steps)
    block_pos = jnp.arange(num_blocks, dtype=jnp.int32)[:, None, None, None]
    residue = jnp.arange(dilation, dtype=jnp.int32)[None, :, None, None]
    source = first_position + (block_pos * block_rows - window_steps + key_pos[None, None]) * dilation + residue
    allowed = inside[None, None] & (source >= 0)
    penalty = -head_slopes[:, None, None] * (distance * dilation).astype(jnp.float32)
    scores = jnp.where(allowed[:, :, None], scores + penalty[None, None], -jnp.inf)
    maxima = jnp.max(scores, axis=-1, keepdims=True)
    weights = jnp.exp(scores - maxima)
    totals = jnp.sum(weights, axis=-1, keepdims=True)
    rounded = lax.optimization_barrier(weights.astype(jnp.bfloat16))
    summed = jnp.einsum("brhqk,bkrhe->bqrhe", rounded.astype(jnp.float32), spans[:, :, :, 1].astype(jnp.float32))
    outputs = summed / jnp.transpose(totals, (0, 3, 1, 2, 4))
    log_part = jnp.transpose((maxima + jnp.log(totals))[..., 0], (0, 3, 1, 2))
    return outputs.reshape(length, heads, depth), log_part.reshape(length, heads)


def combine(query_rows, key_value_rows, head_slopes, first_position):
    length, heads, depth = query_rows.shape
    window_results = [dilated_attention(query_rows, key_value_rows, window_stride, WINDOW_KEY_STEPS, head_slopes, first_position) for window_stride in (1, MIDDLE_DILATION, FAR_DILATION)]
    stacked = jnp.stack([item[1] for item in window_results])
    log_total = jax.nn.logsumexp(stacked, axis=0)
    hidden = jnp.zeros((length, heads, depth), jnp.float32)
    for item in window_results:
        hidden = hidden + jnp.exp(item[1] - log_total)[..., None] * item[0]
    return hidden.reshape(length, heads * depth).astype(jnp.bfloat16), log_total


def reference(tokens, w_query, w_key, w_value, w_out):
    query_rows = jnp.dot(tokens, w_query, preferred_element_type=jnp.float32).astype(jnp.bfloat16)
    keys = jnp.dot(tokens, w_key, preferred_element_type=jnp.float32).astype(jnp.bfloat16)
    values = jnp.dot(tokens, w_value, preferred_element_type=jnp.float32).astype(jnp.bfloat16)
    key_value_rows = jnp.concatenate([keys, values], axis=1)
    padded = jnp.concatenate([jnp.zeros((REACH, key_value_rows.shape[1]), jnp.bfloat16), key_value_rows], axis=0)
    head_slopes = jnp.exp2(-ALIBI_EXP * jnp.arange(1, HEADS + 1, dtype=jnp.float32) / HEADS)

    def segment(index):
        first = index * TOK_DEV
        query_seg = lax.dynamic_slice_in_dim(query_rows, first, TOK_DEV, 0).reshape(TOK_DEV, HEADS, HEAD_DIM)
        keyval_seg = lax.dynamic_slice_in_dim(padded, first, REACH + TOK_DEV, 0)
        return combine(query_seg, keyval_seg, head_slopes, first)

    hidden, log_total = lax.map(segment, jnp.arange(N_SP, dtype=jnp.int32))
    hidden = hidden.reshape(TOKENS, HEADS * HEAD_DIM)
    log_total = log_total.reshape(TOKENS, HEADS)
    width = HEADS * HEAD_DIM // N_TP
    mixed = jnp.zeros((TOKENS, D), jnp.float32)
    for group in range(N_TP):
        partial_value = jnp.dot(hidden[:, group * width:(group + 1) * width], w_out[group * width:(group + 1) * width],
                          preferred_element_type=jnp.float32).astype(jnp.bfloat16)
        mixed = mixed + lax.optimization_barrier(partial_value).astype(jnp.float32)
    return mixed.astype(jnp.bfloat16), log_total.T
```

```python
import functools
import math

import jax
import jax.numpy as jnp
from jax import lax
from jax.experimental import pallas as pl
from jax.experimental.pallas import tpu as pltpu
from jax.sharding import PartitionSpec as P

HEADS = 16
HEAD_DIM = 64
WINDOW_KEY_STEPS = 128
MIDDLE_DILATION = 4
FAR_DILATION = 16
REACH = 2048
ALIBI_EXP = 16.0
LANES = 128
ONES = 16
F32 = jnp.float32
BF16 = jnp.bfloat16
FAR, UP, OWN = 0, 1, 2


def log_multiplicity(distance):
    def window(stride):
        inside = (distance >= 0) & (distance <= WINDOW_KEY_STEPS * stride)
        if stride > 1:
            inside = inside & ((distance & (stride - 1)) == 0)
        return inside.astype(jnp.int32)

    count = window(1) + window(MIDDLE_DILATION) + window(FAR_DILATION)
    return jnp.where(
        count == 3,
        math.log(3.0),
        jnp.where(count == 2, math.log(2.0), jnp.where(count == 1, 0.0, -jnp.inf)),
    ).astype(F32)


def kernel(
    n_sp,
    tokens,
    w_query,
    w_key,
    w_value,
    w_out,
    mixed,
    log_sums,
    xin,
    x,
    wq,
    wk,
    wv,
    wo,
    nat,
    kbuf,
    vbuf,
    vtail,
    qbuf,
    half_perm,
    back_perm,
    tail_pick,
    tab,
    m_ref,
    l_ref,
    acc,
    o_out,
    s_out,
    o_in,
    s_in,
    hid,
    hid_nat,
    logs,
    part_sum,
    part_send,
    part_recv,
    local_sem,
    x_send,
    x_recv,
    kv_send,
    kv_recv,
    q_send,
    q_recv,
    o_send,
    o_recv,
    p_send,
    p_recv,
):
    half, depth = tokens.shape
    length = 2 * half
    n_chunks = kbuf.shape[1]
    classes = MIDDLE_DILATION
    per = length // classes
    per_half = per // 2
    me = lax.axis_index("sp")
    core = lax.axis_index("tp")
    other = 1 - core
    odd = lax.rem(me, 2)
    mate = me + 1 - 2 * odd
    is_even = odd == 0
    is_odd = odd == 1
    has_up = me + 2 < n_sp
    has_far = me + 4 < n_sp
    has_down = me >= 2
    up = jnp.where(has_up, me + 2, me - 2)
    down = jnp.where(has_down, me - 2, me + 2)

    local = [
        pltpu.make_async_copy(tokens, xin, local_sem.at[0]),
        pltpu.make_async_copy(w_key, wk, local_sem.at[1]),
        pltpu.make_async_copy(w_query, wq, local_sem.at[2]),
        pltpu.make_async_copy(w_value, wv, local_sem.at[3]),
        pltpu.make_async_copy(w_out, wo, local_sem.at[4]),
    ]
    for copy in local[:4]:
        copy.start()

    barrier = pltpu.get_barrier_semaphore()
    pl.semaphore_signal(barrier, inc=1, device_id={"tp": other})
    pl.semaphore_signal(barrier, inc=1, device_id={"sp": mate})

    @pl.when(has_up)
    def _():
        pl.semaphore_signal(barrier, inc=1, device_id={"sp": me + 2})

    @pl.when(has_down)
    def _():
        pl.semaphore_signal(barrier, inc=1, device_id={"sp": me - 2})

    half_rows = lax.broadcasted_iota(jnp.int32, (half, half), 0)
    half_cols = lax.broadcasted_iota(jnp.int32, (half, half), 1)
    half_bits = per_half.bit_length() - 1
    half_time = classes * (half_rows & (per_half - 1)) + (half_rows >> half_bits)
    half_perm[...] = (half_time == half_cols).astype(F32).astype(BF16)

    peers = 2 + jnp.where(has_up, 1, 0) + jnp.where(has_down, 1, 0)
    pl.semaphore_wait(barrier, peers)

    local[0].wait()
    x[:, core] = (
        jnp.dot(half_perm[...], xin[...], preferred_element_type=F32)
        .astype(BF16)
        .reshape(classes, per_half, depth)
    )
    x_copy = pltpu.make_async_remote_copy(
        src_ref=x.at[:, core],
        dst_ref=x.at[:, core],
        send_sem=x_send,
        recv_sem=x_recv,
        device_id={"tp": other},
    )
    x_copy.start()

    def project(weights, side):
        rows = x[:, side].reshape(half, depth)
        return jnp.dot(rows, weights[...], preferred_element_type=F32)

    def place_keys(side):
        keys = project(wk, side).astype(BF16)
        for c in range(n_chunks):
            piece = keys[:, c * LANES : (c + 1) * LANES]
            kbuf[0, c, :, side] = piece.reshape(classes, per_half, LANES)

    def place_queries(side):
        queries = (project(wq, side) * HEAD_DIM**-0.5).astype(BF16)
        nat[0, :, side] = queries.reshape(classes, per_half, queries.shape[1])

    def place_values(side):
        values = project(wv, side).astype(BF16)
        nat[1, :, side] = values.reshape(classes, per_half, values.shape[1])

    def key_copy(c, late):
        side = core + late * (1 - 2 * core)
        return pltpu.make_async_remote_copy(
            src_ref=kbuf.at[0, c, :, side],
            dst_ref=kbuf.at[1, c, :, side],
            send_sem=kv_send.at[c, late],
            recv_sem=kv_recv.at[c, late],
            device_id={"sp": mate},
        )

    def value_copy(c):
        return pltpu.make_async_remote_copy(
            src_ref=vbuf.at[0, c],
            dst_ref=vbuf.at[1, c],
            send_sem=kv_send.at[c, 2],
            recv_sem=kv_recv.at[c, 2],
            device_id={"sp": mate},
        )

    def query_copy(c, relay):
        return pltpu.make_async_remote_copy(
            src_ref=qbuf.at[relay, c],
            dst_ref=qbuf.at[relay + 1, c],
            send_sem=q_send.at[relay, c],
            recv_sem=q_recv.at[relay, c],
            device_id={"sp": down},
        )

    def out_copies(kind, c):
        return [
            pltpu.make_async_remote_copy(
                src_ref=src.at[kind, c],
                dst_ref=dst.at[kind, c],
                send_sem=o_send.at[kind, c, i],
                recv_sem=o_recv.at[kind, c, i],
                device_id={"sp": up},
            )
            for i, (src, dst) in enumerate(((o_out, o_in), (s_out, s_in)))
        ]

    def turned(which, c):
        lanes = slice(c * LANES, (c + 1) * LANES)
        return nat[which].reshape(length, n_chunks * LANES)[:, lanes].T

    local[1].wait()
    place_keys(core)
    early = n_chunks // 2
    for c in range(early):
        key_copy(c, 0).start()
    local[2].wait()
    place_queries(core)
    local[3].wait()
    local[4].start()
    place_values(core)

    x_copy.wait()
    place_queries(other)
    for c in range(n_chunks):
        qbuf[0, c] = turned(0, c)
        if c < early:

            @pl.when(has_down)
            def _():
                query_copy(c, 0).start()

    place_keys(other)
    for c in range(early):
        key_copy(c, 1).start()
    place_values(other)
    for c in range(n_chunks):
        if c >= early:
            key_copy(c, 0).start()
            key_copy(c, 1).start()
        vbuf[0, c] = turned(1, c)
        value_copy(c).start()

    key_step = lax.broadcasted_iota(jnp.int32, (per, per), 0)
    query_step = lax.broadcasted_iota(jnp.int32, (per, per), 1)
    tail = per // classes
    tail_bits = tail.bit_length() - 1
    heads_per = LANES // HEAD_DIM

    def slope_of(head):
        number = core * (n_chunks * heads_per) + head + 1
        exponent = jnp.full((1, per), number, jnp.int32).astype(F32)
        return jnp.exp2(exponent * (-ALIBI_EXP / HEADS))

    slopes = [slope_of(h) for h in range(n_chunks * heads_per)]

    def fill(first_row, distance, logc):
        gap = distance.astype(F32)
        rows = pl.ds(pl.multiple_of(first_row, per), per)
        for h in range(n_chunks * heads_per):
            c, j = divmod(h, heads_per)
            tab[c, rows, j * per : (j + 1) * per] = logc - slopes[h] * gap

    steps = classes * (query_step - key_step)
    T0 = 0
    T_CLASS = (2 * classes - 1) * per
    T_TAIL = T_CLASS + classes * per

    @pl.loop(0, 2 * classes - 1)
    def _(e):
        distance = steps + (classes - 1 - e)
        fill(T0 + e * per, distance, log_multiplicity(distance))

    @pl.loop(0, classes)
    def _(e):
        distance = steps + (e + 1) * length
        fill(T_CLASS + e * per, distance, log_multiplicity(distance))

    tail_class = key_step >> tail_bits
    tail_step = (key_step & (tail - 1)) + (per - tail)

    @pl.loop(0, classes)
    def _(r):
        distance = length + classes * (query_step - tail_step) + (r - tail_class)
        logc = jnp.where(tail_class == r, -jnp.inf, log_multiplicity(distance))
        fill(T_TAIL + r * per, distance, logc)

    rows = lax.broadcasted_iota(jnp.int32, (length, length), 0)
    cols = lax.broadcasted_iota(jnp.int32, (length, length), 1)
    per_bits = per.bit_length() - 1
    time_of_row = classes * (rows & (per - 1)) + (rows >> per_bits)
    back_perm[...] = (time_of_row == cols).astype(F32).astype(BF16)
    pick_rows = lax.broadcasted_iota(jnp.int32, (length, per), 0)
    pick_cols = lax.broadcasted_iota(jnp.int32, (length, per), 1)
    pick = (pick_cols >> tail_bits) * per + (per - tail) + (pick_cols & (tail - 1))
    tail_pick[...] = (pick_rows == pick).astype(F32).astype(BF16)

    ones_of = functools.partial(jnp.ones, dtype=BF16)

    def class_part(slot, c, r, table):
        keys = kbuf[slot, c, r].reshape(per, LANES)
        bias = tab[c, table : table + per, :]
        return keys, bias, vbuf[slot, c, :, r * per : (r + 1) * per]

    def gap_table(blocks):
        return T_CLASS + (blocks - 1) * per

    def tail_part(c, r):
        last = tail + per_half - per
        keys = jnp.concatenate(
            [kbuf[1, c, k, 1, per_half - tail :, :] for k in range(classes)], axis=0
        )
        table = T_TAIL + r * per
        return keys, tab[c, table : table + per, :], vtail[c]

    def own_part(c, r):
        first = T0 + (classes - 1 - r) * per
        return (
            kbuf[0, c].reshape(length, LANES),
            tab[c, first : first + length, :],
            vbuf[0, c],
        )

    def attend(item, c, q_slot, parts_of):
        for r in range(classes):
            lanes = slice(r * per, (r + 1) * per)
            parts = parts_of(r)
            first = qbuf[q_slot, c, :HEAD_DIM, lanes]
            second = qbuf[q_slot, c, HEAD_DIM:, lanes]
            blank = jnp.zeros_like(first)
            queries = jnp.concatenate(
                [
                    jnp.concatenate([first, blank], axis=0),
                    jnp.concatenate([blank, second], axis=0),
                ],
                axis=1,
            )
            scores = [
                jnp.dot(keys, queries, preferred_element_type=F32) + bias
                for keys, bias, _ in parts
            ]
            tops = [jnp.max(s, axis=0, keepdims=True) for s in scores]
            top = functools.reduce(jnp.maximum, tops)
            weights = jnp.concatenate(
                [jnp.exp(s - top).astype(BF16) for s in scores], axis=0
            )
            values = jnp.concatenate([v for _, _, v in parts], axis=1)
            count = values.shape[1]
            for j in range(heads_per):
                mine = values[j * HEAD_DIM : (j + 1) * HEAD_DIM]
                summed = jnp.dot(
                    jnp.concatenate([mine, ones_of((ONES, count))], axis=0),
                    weights[:, j * per : (j + 1) * per],
                    preferred_element_type=F32,
                )
                row = slice(r * heads_per + j, r * heads_per + j + 1)
                acc[item, c, j * HEAD_DIM : (j + 1) * HEAD_DIM, lanes] = summed[:HEAD_DIM]
                l_ref[item, c, row, :] = summed[HEAD_DIM : HEAD_DIM + 1]
                m_ref[item, c, row, :] = top[:, j * per : (j + 1) * per]

    def pieces():
        for r in range(classes):
            for j in range(heads_per):
                row = slice(r * heads_per + j, r * heads_per + j + 1)
                dims = slice(j * HEAD_DIM, (j + 1) * HEAD_DIM)
                yield row, dims, slice(r * per, (r + 1) * per)

    def take_in(item, c, kind):
        for copy in out_copies(kind, c):
            copy.wait_recv()
        here, there = m_ref[item, c], s_in[kind, c]
        top = jnp.maximum(here, there)
        keep, gain = jnp.exp(here - top), jnp.exp(there - top)
        m_ref[item, c] = top
        l_ref[item, c] = keep * l_ref[item, c] + gain
        for row, dims, lanes in pieces():
            acc[item, c, dims, lanes] = (
                keep[row] * acc[item, c, dims, lanes]
                + gain[row] * o_in[kind, c, dims, lanes].astype(F32)
            )

    def level(item, c, out):
        total = l_ref[item, c]
        scale = 1.0 / total
        for row, dims, lanes in pieces():
            out[dims, lanes] = (acc[item, c, dims, lanes] * scale[row]).astype(BF16)
        return m_ref[item, c] + jnp.log(total)

    def emit(item, c):
        s_out[item, c] = level(item, c, o_out.at[item, c])
        for copy in out_copies(item, c):
            copy.start()

    def finish(c):
        @pl.when(has_down)
        def _():
            take_in(OWN, c, UP)

        logs[c] = level(OWN, c, hid.at[c])
        hid_nat[c] = (
            jnp.dot(hid[c], back_perm[...], preferred_element_type=F32).astype(BF16).T
        )

    def merge_up(c):
        @pl.when(has_up)
        def _():
            @pl.when(has_down)
            def _():
                take_in(UP, c, FAR)

            emit(UP, c)

    def step(c):
        @pl.when(has_up)
        def _():
            query_copy(c, 0).wait_recv()

            @pl.when(has_down)
            def _():
                query_copy(c, 1).start()

        @pl.when(has_down & (c + early < n_chunks))
        def _():
            query_copy(c + early, 0).start()

        key_copy(c, 0).wait_recv()
        key_copy(c, 1).wait_recv()
        value_copy(c).wait_recv()
        vtail[c] = jnp.dot(
            vbuf[1, c], tail_pick[...], preferred_element_type=F32
        ).astype(BF16)

        @pl.when(has_up & is_even)
        def _():
            attend(
                UP,
                c,
                1,
                lambda r: [
                    class_part(0, c, r, gap_table(2)),
                    class_part(1, c, r, gap_table(1)),
                    tail_part(c, r),
                ],
            )

        @pl.when(has_up & is_odd)
        def _():
            attend(
                UP,
                c,
                1,
                lambda r: [
                    class_part(0, c, r, gap_table(2)),
                    class_part(1, c, r, gap_table(3)),
                ],
            )

        @pl.when(is_even)
        def _():
            attend(OWN, c, 0, lambda r: [own_part(c, r)])

        @pl.when(is_odd)
        def _():
            attend(
                OWN,
                c,
                0,
                lambda r: [
                    own_part(c, r),
                    class_part(1, c, r, gap_table(1)),
                    tail_part(c, r),
                ],
            )

        @pl.when(c >= 1)
        def _():
            merge_up(c - 1)

        @pl.when(has_far)
        def _():
            query_copy(c, 1).wait_recv()

            @pl.when(is_even)
            def _():
                attend(
                    FAR,
                    c,
                    2,
                    lambda r: [
                        class_part(0, c, r, gap_table(4)),
                        class_part(1, c, r, gap_table(3)),
                    ],
                )

            @pl.when(is_odd)
            def _():
                attend(FAR, c, 2, lambda r: [class_part(0, c, r, gap_table(4))])

            emit(FAR, c)

        @pl.when(c >= 2)
        def _():
            finish(c - 2)

    @pl.loop(0, n_chunks)
    def _(c):
        step(c)

    local[4].wait()
    out_width = wo.shape[1]
    n_parts = p_send.shape[0]
    part_width = out_width // n_parts
    done = n_chunks - 2

    def all_parts():
        return [slice(p * part_width, (p + 1) * part_width) for p in range(n_parts)]

    sofar = jnp.concatenate([hid_nat[c] for c in range(done)], axis=1)
    for lanes in all_parts():
        part_sum[:, lanes] = jnp.dot(
            sofar, wo[: done * LANES, lanes], preferred_element_type=F32
        )
    merge_up(n_chunks - 1)
    for c in range(done, n_chunks):
        finish(c)

    part_copies = [
        pltpu.make_async_remote_copy(
            src_ref=part_send.at[:, lanes],
            dst_ref=part_recv.at[:, lanes],
            send_sem=p_send.at[p],
            recv_sem=p_recv.at[p],
            device_id={"tp": other},
        )
        for p, lanes in enumerate(all_parts())
    ]
    my_rows = pl.ds(pl.multiple_of(core * half, half), half)
    their_rows = pl.ds(pl.multiple_of(other * half, half), half)

    def partial(rows_, lanes):
        late = jnp.concatenate([hid_nat[c, rows_, :] for c in range(done, n_chunks)], axis=1)
        rest = jnp.dot(late, wo[done * LANES :, lanes], preferred_element_type=F32)
        return (part_sum[rows_, lanes] + rest).astype(BF16)

    for p, lanes in enumerate(all_parts()):
        part_send[:, lanes] = partial(their_rows, lanes)
        part_copies[p].start()

    ordered = jnp.concatenate(
        [
            jnp.concatenate(
                [logs[c, r * heads_per + j : r * heads_per + j + 1, :] for r in range(classes)],
                axis=1,
            )
            for c in range(n_chunks)
            for j in range(heads_per)
        ],
        axis=0,
    )
    high = ordered.astype(BF16)
    left = ordered - high.astype(F32)
    middle = left.astype(BF16)
    low = (left - middle.astype(F32)).astype(BF16)
    log_sums[...] = functools.reduce(
        jnp.add,
        [
            jnp.dot(piece, back_perm[...], preferred_element_type=F32)
            for piece in (low, middle, high)
        ],
    )
    for p, lanes in enumerate(all_parts()):
        own = partial(my_rows, lanes)
        part_copies[p].wait_recv()
        mixed[:, lanes] = (own.astype(F32) + part_recv[:, lanes].astype(F32)).astype(BF16)

    for copy in part_copies:
        copy.wait_send()

    @pl.loop(0, n_chunks)
    def _(c):
        key_copy(c, 0).wait_send()
        key_copy(c, 1).wait_send()
        value_copy(c).wait_send()

        @pl.when(has_down)
        def _():
            query_copy(c, 0).wait_send()

        @pl.when(has_down & has_up)
        def _():
            query_copy(c, 1).wait_send()

        @pl.when(has_far)
        def _():
            for copy in out_copies(FAR, c):
                copy.wait_send()

        @pl.when(has_up)
        def _():
            for copy in out_copies(UP, c):
                copy.wait_send()


def body(n_sp, tokens, w_query, w_key, w_value, w_out):
    half, depth = tokens.shape
    length = 2 * half
    width = w_query.shape[1]
    out_width = w_out.shape[1]
    heads = width // HEAD_DIM
    chunks = width // LANES
    assert REACH == MIDDLE_DILATION * length and n_sp % 2 == 0
    per = length // MIDDLE_DILATION
    stats = MIDDLE_DILATION * (LANES // HEAD_DIM)
    parts = max(1, out_width // 512)
    tables = (4 * MIDDLE_DILATION - 1) * per
    hbm = pl.BlockSpec(memory_space=pl.ANY)
    vmem = pl.BlockSpec(memory_space=pltpu.VMEM)
    dma = pltpu.SemaphoreType.DMA
    return pl.pallas_call(
        functools.partial(kernel, n_sp),
        out_shape=(
            jax.ShapeDtypeStruct((half, out_width), BF16),
            jax.ShapeDtypeStruct((heads, length), F32),
        ),
        in_specs=[hbm] * 5,
        out_specs=(vmem, vmem),
        scratch_shapes=[
            pltpu.VMEM((half, depth), BF16),
            pltpu.VMEM((MIDDLE_DILATION, 2, per // 2, depth), BF16),
            pltpu.VMEM((depth, width), BF16),
            pltpu.VMEM((depth, width), BF16),
            pltpu.VMEM((depth, width), BF16),
            pltpu.VMEM((width, out_width), BF16),
            pltpu.VMEM((2, MIDDLE_DILATION, 2, per // 2, width), BF16),
            pltpu.VMEM((2, chunks, MIDDLE_DILATION, 2, per // 2, LANES), BF16),
            pltpu.VMEM((2, chunks, LANES, length), BF16),
            pltpu.VMEM((chunks, LANES, per), BF16),
            pltpu.VMEM((3, chunks, LANES, length), BF16),
            pltpu.VMEM((half, half), BF16),
            pltpu.VMEM((length, length), BF16),
            pltpu.VMEM((length, per), BF16),
            pltpu.VMEM((chunks, tables, 2 * per), F32),
            pltpu.VMEM((3, chunks, stats, per), F32),
            pltpu.VMEM((3, chunks, stats, per), F32),
            pltpu.VMEM((3, chunks, LANES, length), F32),
            pltpu.VMEM((2, chunks, LANES, length), BF16),
            pltpu.VMEM((2, chunks, stats, per), F32),
            pltpu.VMEM((2, chunks, LANES, length), BF16),
            pltpu.VMEM((2, chunks, stats, per), F32),
            pltpu.VMEM((chunks, LANES, length), BF16),
            pltpu.VMEM((chunks, length, LANES), BF16),
            pltpu.VMEM((chunks, stats, per), F32),
            pltpu.VMEM((length, out_width), F32),
            pltpu.VMEM((half, out_width), BF16),
            pltpu.VMEM((half, out_width), BF16),
            dma((5,)),
            dma,
            dma,
            dma((chunks, 3)),
            dma((chunks, 3)),
            dma((2, chunks)),
            dma((2, chunks)),
            dma((2, chunks, 2)),
            dma((2, chunks, 2)),
            dma((parts,)),
            dma((parts,)),
        ],
        compiler_params=pltpu.CompilerParams(
            collective_id=0, has_side_effects=True, vmem_limit_bytes=60 * 1024 * 1024
        ),
        name="dilated_layer",
    )(tokens, w_query, w_key, w_value, w_out)


def solution(mesh):
    in_specs = (
        P(("grp", "sp", "tp"), None),
        P(None, "tp"),
        P(None, "tp"),
        P(None, "tp"),
        P("tp", None),
    )
    out_specs = (P(("grp", "sp", "tp"), None), P("tp", ("grp", "sp")))
    return jax.shard_map(
        functools.partial(body, mesh.shape["sp"]),
        mesh=mesh,
        in_specs=in_specs,
        out_specs=out_specs,
        check_vma=False,
    )
```

```python
import functools
import math

import jax
import jax.numpy as jnp
from jax import lax
from jax.experimental import pallas as pl
from jax.experimental.pallas import tpu as pltpu
from jax.sharding import PartitionSpec as P

HEADS = 16
HEAD_DIM = 64
WINDOW_KEY_STEPS = 128
MIDDLE_DILATION = 4
FAR_DILATION = 16
REACH = 2048
ALIBI_EXP = 16.0
LANES = 128
ONES = 16
F32 = jnp.float32
BF16 = jnp.bfloat16
FAR, UP, OWN = 0, 1, 2


def log_multiplicity(distance):
    def window(stride):
        inside = (distance >= 0) & (distance <= WINDOW_KEY_STEPS * stride)
        if stride > 1:
            inside = inside & ((distance & (stride - 1)) == 0)
        return inside.astype(jnp.int32)

    count = window(1) + window(MIDDLE_DILATION) + window(FAR_DILATION)
    return jnp.where(
        count == 3,
        math.log(3.0),
        jnp.where(count == 2, math.log(2.0), jnp.where(count == 1, 0.0, -jnp.inf)),
    ).astype(F32)


def kernel(
    n_sp,
    tokens,
    w_query,
    w_key,
    w_value,
    w_out,
    mixed,
    log_sums,
    xin,
    x,
    wq,
    wk,
    wv,
    wo,
    nat,
    kbuf,
    vbuf,
    vtail,
    qbuf,
    half_perm,
    back_perm,
    tail_pick,
    tab,
    m_ref,
    l_ref,
    acc,
    o_out,
    s_out,
    o_in,
    s_in,
    hid,
    hid_nat,
    logs,
    hid_in,
    part_sum,
    local_sem,
    x_send,
    x_recv,
    kv_send,
    kv_recv,
    q_send,
    q_recv,
    o_send,
    o_recv,
    h_send,
    h_recv,
    w_send,
    w_recv,
):
    half, depth = tokens.shape
    length = 2 * half
    n_chunks = kbuf.shape[1]
    classes = MIDDLE_DILATION
    per = length // classes
    per_half = per // 2
    me = lax.axis_index("sp")
    core = lax.axis_index("tp")
    other = 1 - core
    odd = lax.rem(me, 2)
    mate = me + 1 - 2 * odd
    is_even = odd == 0
    is_odd = odd == 1
    has_up = me + 2 < n_sp
    has_far = me + 4 < n_sp
    has_down = me >= 2
    up = jnp.where(has_up, me + 2, me - 2)
    down = jnp.where(has_down, me - 2, me + 2)

    local = [
        pltpu.make_async_copy(tokens, xin, local_sem.at[0]),
        pltpu.make_async_copy(w_key, wk, local_sem.at[1]),
        pltpu.make_async_copy(w_query, wq, local_sem.at[2]),
        pltpu.make_async_copy(w_value, wv, local_sem.at[3]),
        pltpu.make_async_copy(w_out, wo.at[0], local_sem.at[4]),
    ]
    for copy in local[:4]:
        copy.start()

    barrier = pltpu.get_barrier_semaphore()
    pl.semaphore_signal(barrier, inc=1, device_id={"tp": other})
    pl.semaphore_signal(barrier, inc=1, device_id={"sp": mate})

    @pl.when(has_up)
    def _():
        pl.semaphore_signal(barrier, inc=1, device_id={"sp": me + 2})

    @pl.when(has_down)
    def _():
        pl.semaphore_signal(barrier, inc=1, device_id={"sp": me - 2})

    half_rows = lax.broadcasted_iota(jnp.int32, (half, half), 0)
    half_cols = lax.broadcasted_iota(jnp.int32, (half, half), 1)
    half_bits = per_half.bit_length() - 1
    half_time = classes * (half_rows & (per_half - 1)) + (half_rows >> half_bits)
    half_perm[...] = (half_time == half_cols).astype(F32).astype(BF16)

    local[0].wait()
    x[:, core] = (
        jnp.dot(half_perm[...], xin[...], preferred_element_type=F32)
        .astype(BF16)
        .reshape(classes, per_half, depth)
    )
    peers = 2 + jnp.where(has_up, 1, 0) + jnp.where(has_down, 1, 0)
    pl.semaphore_wait(barrier, peers)
    x_copy = pltpu.make_async_remote_copy(
        src_ref=x.at[:, core],
        dst_ref=x.at[:, core],
        send_sem=x_send,
        recv_sem=x_recv,
        device_id={"tp": other},
    )
    x_copy.start()
    my_rows = pl.ds(pl.multiple_of(core * half, half), half)
    their_rows = pl.ds(pl.multiple_of(other * half, half), half)

    def project(weights, side):
        rows = x[:, side].reshape(half, depth)
        return jnp.dot(rows, weights[...], preferred_element_type=F32)

    def place_keys(side):
        keys = project(wk, side).astype(BF16)
        for c in range(n_chunks):
            piece = keys[:, c * LANES : (c + 1) * LANES]
            kbuf[0, c, :, side] = piece.reshape(classes, per_half, LANES)

    def place_queries(side):
        queries = (project(wq, side) * HEAD_DIM**-0.5).astype(BF16)
        nat[0, :, side] = queries.reshape(classes, per_half, queries.shape[1])

    def place_values(side):
        values = project(wv, side).astype(BF16)
        nat[1, :, side] = values.reshape(classes, per_half, values.shape[1])

    def key_copy(c, late):
        side = core + late * (1 - 2 * core)
        return pltpu.make_async_remote_copy(
            src_ref=kbuf.at[0, c, :, side],
            dst_ref=kbuf.at[1, c, :, side],
            send_sem=kv_send.at[c, late],
            recv_sem=kv_recv.at[c, late],
            device_id={"sp": mate},
        )

    def value_copy(c):
        return pltpu.make_async_remote_copy(
            src_ref=vbuf.at[0, c],
            dst_ref=vbuf.at[1, c],
            send_sem=kv_send.at[c, 2],
            recv_sem=kv_recv.at[c, 2],
            device_id={"sp": mate},
        )

    def query_copy(s, relay):
        return pltpu.make_async_remote_copy(
            src_ref=qbuf.at[relay, s],
            dst_ref=qbuf.at[relay + 1, s],
            send_sem=q_send.at[relay, s],
            recv_sem=q_recv.at[relay, s],
            device_id={"sp": down},
        )

    def out_copies(kind, s):
        return [
            pltpu.make_async_remote_copy(
                src_ref=src.at[kind, s],
                dst_ref=dst.at[kind, s],
                send_sem=o_send.at[kind, s, i],
                recv_sem=o_recv.at[kind, s, i],
                device_id={"sp": up},
            )
            for i, (src, dst) in enumerate(((o_out, o_in), (s_out, s_in)))
        ]

    def hidden_copy(c):
        return pltpu.make_async_remote_copy(
            src_ref=hid_nat.at[c, their_rows],
            dst_ref=hid_in.at[c],
            send_sem=h_send.at[c],
            recv_sem=h_recv.at[c],
            device_id={"tp": other},
        )

    w_copy = pltpu.make_async_remote_copy(
        src_ref=w_out,
        dst_ref=wo.at[1],
        send_sem=w_send,
        recv_sem=w_recv,
        device_id={"tp": other},
    )

    def turned(which, c):
        lanes = slice(c * LANES, (c + 1) * LANES)
        return nat[which].reshape(length, n_chunks * LANES)[:, lanes].T

    local[1].wait()
    place_keys(core)
    early = n_chunks // 2
    for c in range(early):
        key_copy(c, 0).start()
    local[2].wait()
    place_queries(core)
    local[3].wait()
    local[4].start()
    place_values(core)

    x_copy.wait()
    place_queries(other)
    groups = 2
    wide = length // groups
    for c in range(n_chunks):
        queries = turned(0, c)
        for g in range(groups):
            qbuf[0, c * groups + g] = queries[:, g * wide : (g + 1) * wide]
            if c == 0:

                @pl.when(has_down)
                def _():
                    query_copy(g, 0).start()

    place_keys(other)
    for c in range(early):
        key_copy(c, 1).start()
    place_values(other)
    for c in range(n_chunks):
        if c >= early:
            key_copy(c, 0).start()
            key_copy(c, 1).start()
        vbuf[0, c] = turned(1, c)
        value_copy(c).start()
    w_copy.start()

    key_step = lax.broadcasted_iota(jnp.int32, (per, per), 0)
    query_step = lax.broadcasted_iota(jnp.int32, (per, per), 1)
    tail = per // classes
    tail_bits = tail.bit_length() - 1
    heads_per = LANES // HEAD_DIM

    def slope_of(head):
        number = core * (n_chunks * heads_per) + head + 1
        exponent = jnp.full((1, per), number, jnp.int32).astype(F32)
        return jnp.exp2(exponent * (-ALIBI_EXP / HEADS))

    slopes = [slope_of(h) for h in range(n_chunks * heads_per)]

    def fill(first_row, distance, logc):
        gap = distance.astype(F32)
        rows = pl.ds(pl.multiple_of(first_row, per), per)
        for h in range(n_chunks * heads_per):
            c, j = divmod(h, heads_per)
            tab[c, rows, j * per : (j + 1) * per] = logc - slopes[h] * gap

    steps = classes * (query_step - key_step)
    T0 = 0
    T_CLASS = (2 * classes - 1) * per
    T_TAIL = T_CLASS + classes * per

    @pl.loop(0, 2 * classes - 1)
    def _(e):
        distance = steps + (classes - 1 - e)
        fill(T0 + e * per, distance, log_multiplicity(distance))

    @pl.loop(0, classes)
    def _(e):
        distance = steps + (e + 1) * length
        fill(T_CLASS + e * per, distance, log_multiplicity(distance))

    tail_class = key_step >> tail_bits
    tail_step = (key_step & (tail - 1)) + (per - tail)

    @pl.loop(0, classes)
    def _(r):
        distance = length + classes * (query_step - tail_step) + (r - tail_class)
        logc = jnp.where(tail_class == r, -jnp.inf, log_multiplicity(distance))
        fill(T_TAIL + r * per, distance, logc)

    rows = lax.broadcasted_iota(jnp.int32, (length, length), 0)
    cols = lax.broadcasted_iota(jnp.int32, (length, length), 1)
    per_bits = per.bit_length() - 1
    time_of_row = classes * (rows & (per - 1)) + (rows >> per_bits)
    back_perm[...] = (time_of_row == cols).astype(F32).astype(BF16)
    pick_rows = lax.broadcasted_iota(jnp.int32, (length, per), 0)
    pick_cols = lax.broadcasted_iota(jnp.int32, (length, per), 1)
    pick = (pick_cols >> tail_bits) * per + (per - tail) + (pick_cols & (tail - 1))
    tail_pick[...] = (pick_rows == pick).astype(F32).astype(BF16)

    ones_of = functools.partial(jnp.ones, dtype=BF16)

    def class_part(slot, c, r, table):
        keys = kbuf[slot, c, r].reshape(per, LANES)
        bias = tab[c, table : table + per, :]
        return keys, bias, vbuf[slot, c, :, r * per : (r + 1) * per]

    def gap_table(blocks):
        return T_CLASS + (blocks - 1) * per

    def tail_part(c, r):
        keys = jnp.concatenate(
            [kbuf[1, c, k, 1, per_half - tail :, :] for k in range(classes)], axis=0
        )
        table = T_TAIL + r * per
        return keys, tab[c, table : table + per, :], vtail[c]

    def own_part(c, r):
        first = T0 + (classes - 1 - r) * per
        return (
            kbuf[0, c].reshape(length, LANES),
            tab[c, first : first + length, :],
            vbuf[0, c],
        )

    per_group = classes // groups

    def attend(item, c, g, q_slot, parts_of):
        piece = c * groups + g
        for i in range(per_group):
            r = g * per_group + i
            lanes = slice(i * per, (i + 1) * per)
            parts = parts_of(r)
            first = qbuf[q_slot, piece, :HEAD_DIM, lanes]
            second = qbuf[q_slot, piece, HEAD_DIM:, lanes]
            blank = jnp.zeros_like(first)
            queries = jnp.concatenate(
                [
                    jnp.concatenate([first, blank], axis=0),
                    jnp.concatenate([blank, second], axis=0),
                ],
                axis=1,
            )
            scores = [
                jnp.dot(keys, queries, preferred_element_type=F32) + bias
                for keys, bias, _ in parts
            ]
            tops = [jnp.max(s, axis=0, keepdims=True) for s in scores]
            top = functools.reduce(jnp.maximum, tops)
            weights = jnp.concatenate(
                [jnp.exp(s - top).astype(BF16) for s in scores], axis=0
            )
            values = jnp.concatenate([v for _, _, v in parts], axis=1)
            count = values.shape[1]
            for j in range(heads_per):
                mine = values[j * HEAD_DIM : (j + 1) * HEAD_DIM]
                summed = jnp.dot(
                    jnp.concatenate([mine, ones_of((ONES, count))], axis=0),
                    weights[:, j * per : (j + 1) * per],
                    preferred_element_type=F32,
                )
                row = slice(i * heads_per + j, i * heads_per + j + 1)
                acc[item, piece, j * HEAD_DIM : (j + 1) * HEAD_DIM, lanes] = summed[:HEAD_DIM]
                l_ref[item, piece, row, :] = summed[HEAD_DIM : HEAD_DIM + 1]
                m_ref[item, piece, row, :] = top[:, j * per : (j + 1) * per]

    def blocks():
        for i in range(per_group):
            for j in range(heads_per):
                row = slice(i * heads_per + j, i * heads_per + j + 1)
                dims = slice(j * HEAD_DIM, (j + 1) * HEAD_DIM)
                yield row, dims, slice(i * per, (i + 1) * per)

    def take_in(item, s, kind):
        for copy in out_copies(kind, s):
            copy.wait_recv()
        here, there = m_ref[item, s], s_in[kind, s]
        top = jnp.maximum(here, there)
        keep, gain = jnp.exp(here - top), jnp.exp(there - top)
        m_ref[item, s] = top
        l_ref[item, s] = keep * l_ref[item, s] + gain
        for row, dims, lanes in blocks():
            acc[item, s, dims, lanes] = (
                keep[row] * acc[item, s, dims, lanes]
                + gain[row] * o_in[kind, s, dims, lanes].astype(F32)
            )

    def level(item, s, out):
        total = l_ref[item, s]
        scale = 1.0 / total
        for row, dims, lanes in blocks():
            out[dims, lanes] = (acc[item, s, dims, lanes] * scale[row]).astype(BF16)
        return m_ref[item, s] + jnp.log(total)

    def emit(item, s):
        s_out[item, s] = level(item, s, o_out.at[item, s])
        for copy in out_copies(item, s):
            copy.start()

    def finish(c, g):
        piece = c * groups + g

        @pl.when(has_down)
        def _():
            take_in(OWN, piece, UP)

        logs[piece] = level(OWN, piece, hid.at[c, :, g * wide : (g + 1) * wide])
        if g == groups - 1:
            hid_nat[c] = (
                jnp.dot(hid[c], back_perm[...], preferred_element_type=F32).astype(BF16).T
            )
            hidden_copy(c).start()

    n_pieces = n_chunks * groups

    def merge_up(s):
        @pl.when(has_up & (s >= 0) & (s < n_pieces))
        def _():
            @pl.when(has_down)
            def _():
                take_in(UP, s, FAR)

            emit(UP, s)

    def pass_on(s):
        @pl.when(has_up & (s < n_pieces))
        def _():
            query_copy(s, 0).wait_recv()

            @pl.when(has_down)
            def _():
                query_copy(s, 1).start()

        @pl.when(has_down & (s + groups < n_pieces))
        def _():
            query_copy(s + groups, 0).start()

    def attend_all(c, g):
        if g == 0:
            key_copy(c, 0).wait_recv()
            key_copy(c, 1).wait_recv()
            value_copy(c).wait_recv()
            vtail[c] = jnp.dot(
                vbuf[1, c], tail_pick[...], preferred_element_type=F32
            ).astype(BF16)

        @pl.when(has_up & is_even)
        def _():
            attend(
                UP,
                c,
                g,
                1,
                lambda r: [
                    class_part(0, c, r, gap_table(2)),
                    class_part(1, c, r, gap_table(1)),
                    tail_part(c, r),
                ],
            )

        @pl.when(has_up & is_odd)
        def _():
            attend(
                UP,
                c,
                g,
                1,
                lambda r: [
                    class_part(0, c, r, gap_table(2)),
                    class_part(1, c, r, gap_table(3)),
                ],
            )

        @pl.when(is_even)
        def _():
            attend(OWN, c, g, 0, lambda r: [own_part(c, r)])

        @pl.when(is_odd)
        def _():
            attend(
                OWN,
                c,
                g,
                0,
                lambda r: [
                    own_part(c, r),
                    class_part(1, c, r, gap_table(1)),
                    tail_part(c, r),
                ],
            )

        @pl.when(has_far)
        def _():
            piece = c * groups + g
            query_copy(piece, 1).wait_recv()

            @pl.when(is_even)
            def _():
                attend(
                    FAR,
                    c,
                    g,
                    2,
                    lambda r: [
                        class_part(0, c, r, gap_table(4)),
                        class_part(1, c, r, gap_table(3)),
                    ],
                )

            @pl.when(is_odd)
            def _():
                attend(FAR, c, g, 2, lambda r: [class_part(0, c, r, gap_table(4))])

            emit(FAR, piece)

    @pl.loop(0, n_chunks + 1)
    def _(c):
        for g in range(groups):
            beat = c * groups + g
            pass_on(beat)
            merge_up(beat - 3)
            if g == 0:

                @pl.when(c >= 1)
                def _():
                    attend_all(c - 1, groups - 1)

            else:

                @pl.when(c < n_chunks)
                def _():
                    attend_all(c, g - 1)

            @pl.when(c >= 2)
            def _():
                finish(c - 2, g)

    out_width = wo.shape[2]
    n_parts = max(1, out_width // 512)
    part_width = out_width // n_parts
    done = n_chunks - 1

    def all_parts():
        return [slice(p * part_width, (p + 1) * part_width) for p in range(n_parts)]

    def spread(first, last_):
        return jnp.concatenate(
            [hid_nat[c, my_rows, :] for c in range(first, last_)]
            + [hid_in[c] for c in range(first, last_)],
            axis=1,
        )

    def weights_of(first, last_, lanes):
        rows_ = slice(first * LANES, last_ * LANES)
        return jnp.concatenate([wo[0, rows_, lanes], wo[1, rows_, lanes]], axis=0)

    merge_up(n_pieces - 1)
    local[4].wait()
    w_copy.wait()
    for c in range(done):
        hidden_copy(c).wait_recv()
    sofar = spread(0, done)
    for lanes in all_parts():
        part_sum[:, lanes] = jnp.dot(
            sofar, weights_of(0, done, lanes), preferred_element_type=F32
        )
    for g in range(groups):
        finish(done, g)

    ordered = jnp.concatenate(
        [
            jnp.concatenate(
                [
                    logs[c * groups + g, i * heads_per + j : i * heads_per + j + 1, :]
                    for g in range(groups)
                    for i in range(per_group)
                ],
                axis=1,
            )
            for c in range(n_chunks)
            for j in range(heads_per)
        ],
        axis=0,
    )
    high = ordered.astype(BF16)
    left = ordered - high.astype(F32)
    middle = left.astype(BF16)
    low = (left - middle.astype(F32)).astype(BF16)
    log_sums[...] = functools.reduce(
        jnp.add,
        [
            jnp.dot(piece, back_perm[...], preferred_element_type=F32)
            for piece in (low, middle, high)
        ],
    )
    for c in range(done, n_chunks):
        hidden_copy(c).wait_recv()
    late = spread(done, n_chunks)
    for lanes in all_parts():
        rest = jnp.dot(late, weights_of(done, n_chunks, lanes), preferred_element_type=F32)
        mixed[:, lanes] = (part_sum[:, lanes] + rest).astype(BF16)

    @pl.loop(0, n_chunks)
    def _(c):
        key_copy(c, 0).wait_send()
        key_copy(c, 1).wait_send()
        value_copy(c).wait_send()
        hidden_copy(c).wait_send()

    @pl.loop(0, n_pieces)
    def _(s):
        @pl.when(has_down)
        def _():
            query_copy(s, 0).wait_send()

        @pl.when(has_down & has_up)
        def _():
            query_copy(s, 1).wait_send()

        @pl.when(has_far)
        def _():
            for copy in out_copies(FAR, s):
                copy.wait_send()

        @pl.when(has_up)
        def _():
            for copy in out_copies(UP, s):
                copy.wait_send()


def body(n_sp, tokens, w_query, w_key, w_value, w_out):
    half, depth = tokens.shape
    length = 2 * half
    width = w_query.shape[1]
    out_width = w_out.shape[1]
    heads = width // HEAD_DIM
    chunks = width // LANES
    assert REACH == MIDDLE_DILATION * length and n_sp % 2 == 0
    per = length // MIDDLE_DILATION
    groups = 2
    pieces, wide = chunks * groups, length // groups
    stats = MIDDLE_DILATION // groups * (LANES // HEAD_DIM)
    tables = (4 * MIDDLE_DILATION - 1) * per
    hbm = pl.BlockSpec(memory_space=pl.ANY)
    vmem = pl.BlockSpec(memory_space=pltpu.VMEM)
    dma = pltpu.SemaphoreType.DMA
    return pl.pallas_call(
        functools.partial(kernel, n_sp),
        out_shape=(
            jax.ShapeDtypeStruct((half, out_width), BF16),
            jax.ShapeDtypeStruct((heads, length), F32),
        ),
        in_specs=[hbm] * 5,
        out_specs=(vmem, vmem),
        scratch_shapes=[
            pltpu.VMEM((half, depth), BF16),
            pltpu.VMEM((MIDDLE_DILATION, 2, per // 2, depth), BF16),
            pltpu.VMEM((depth, width), BF16),
            pltpu.VMEM((depth, width), BF16),
            pltpu.VMEM((depth, width), BF16),
            pltpu.VMEM((2, width, out_width), BF16),
            pltpu.VMEM((2, MIDDLE_DILATION, 2, per // 2, width), BF16),
            pltpu.VMEM((2, chunks, MIDDLE_DILATION, 2, per // 2, LANES), BF16),
            pltpu.VMEM((2, chunks, LANES, length), BF16),
            pltpu.VMEM((chunks, LANES, per), BF16),
            pltpu.VMEM((3, pieces, LANES, wide), BF16),
            pltpu.VMEM((half, half), BF16),
            pltpu.VMEM((length, length), BF16),
            pltpu.VMEM((length, per), BF16),
            pltpu.VMEM((chunks, tables, 2 * per), F32),
            pltpu.VMEM((3, pieces, stats, per), F32),
            pltpu.VMEM((3, pieces, stats, per), F32),
            pltpu.VMEM((3, pieces, LANES, wide), F32),
            pltpu.VMEM((2, pieces, LANES, wide), BF16),
            pltpu.VMEM((2, pieces, stats, per), F32),
            pltpu.VMEM((2, pieces, LANES, wide), BF16),
            pltpu.VMEM((2, pieces, stats, per), F32),
            pltpu.VMEM((chunks, LANES, length), BF16),
            pltpu.VMEM((chunks, length, LANES), BF16),
            pltpu.VMEM((pieces, stats, per), F32),
            pltpu.VMEM((chunks, half, LANES), BF16),
            pltpu.VMEM((half, out_width), F32),
            dma((5,)),
            dma,
            dma,
            dma((chunks, 3)),
            dma((chunks, 3)),
            dma((2, pieces)),
            dma((2, pieces)),
            dma((2, pieces, 2)),
            dma((2, pieces, 2)),
            dma((chunks,)),
            dma((chunks,)),
            dma,
            dma,
        ],
        compiler_params=pltpu.CompilerParams(
            collective_id=0, has_side_effects=True, vmem_limit_bytes=52 * 1024 * 1024
        ),
        name="dilated_layer",
    )(tokens, w_query, w_key, w_value, w_out)


def solution(mesh):
    in_specs = (
        P(("grp", "sp", "tp"), None),
        P(None, "tp"),
        P(None, "tp"),
        P(None, "tp"),
        P("tp", None),
    )
    out_specs = (P(("grp", "sp", "tp"), None), P("tp", ("grp", "sp")))
    return jax.shard_map(
        functools.partial(body, mesh.shape["sp"]),
        mesh=mesh,
        in_specs=in_specs,
        out_specs=out_specs,
        check_vma=False,
    )
```

```python
import functools
import math

import jax
import jax.numpy as jnp
from jax import lax
from jax.experimental import pallas as pl
from jax.experimental.pallas import tpu as pltpu
from jax.sharding import PartitionSpec as P

HEADS = 16
HEAD_DIM = 64
WINDOW_KEY_STEPS = 128
MIDDLE_DILATION = 4
FAR_DILATION = 16
REACH = 2048
ALIBI_EXP = 16.0
LANES = 128
ONES = 16
F32 = jnp.float32
BF16 = jnp.bfloat16
FAR, UP, OWN = 0, 1, 2


def log_multiplicity(distance):
    def window(stride):
        inside = (distance >= 0) & (distance <= WINDOW_KEY_STEPS * stride)
        if stride > 1:
            inside = inside & ((distance & (stride - 1)) == 0)
        return inside.astype(jnp.int32)

    count = window(1) + window(MIDDLE_DILATION) + window(FAR_DILATION)
    return jnp.where(
        count == 3,
        math.log(3.0),
        jnp.where(count == 2, math.log(2.0), jnp.where(count == 1, 0.0, -jnp.inf)),
    ).astype(F32)


def kernel(
    n_sp,
    tokens,
    w_query,
    w_key,
    w_value,
    w_out,
    mixed,
    log_sums,
    xin,
    x,
    wq,
    wk,
    wv,
    wo,
    nat,
    kbuf,
    vbuf,
    vtail,
    qbuf,
    half_perm,
    back_perm,
    tail_pick,
    tab,
    m_ref,
    l_ref,
    acc,
    o_out,
    s_out,
    o_in,
    s_in,
    hid,
    hid_nat,
    logs,
    hid_in,
    part_sum,
    local_sem,
    x_send,
    x_recv,
    kv_send,
    kv_recv,
    q_send,
    q_recv,
    o_send,
    o_recv,
    h_send,
    h_recv,
    w_send,
    w_recv,
):
    half, depth = tokens.shape
    length = 2 * half
    n_chunks = kbuf.shape[1]
    classes = MIDDLE_DILATION
    per = length // classes
    per_half = per // 2
    me = lax.axis_index("sp")
    core = lax.axis_index("tp")
    other = 1 - core
    odd = lax.rem(me, 2)
    mate = me + 1 - 2 * odd
    is_even = odd == 0
    is_odd = odd == 1
    has_up = me + 2 < n_sp
    has_far = me + 4 < n_sp
    has_down = me >= 2
    up = jnp.where(has_up, me + 2, me - 2)
    down = jnp.where(has_down, me - 2, me + 2)

    local = [
        pltpu.make_async_copy(tokens, xin, local_sem.at[0]),
        pltpu.make_async_copy(w_key, wk, local_sem.at[1]),
        pltpu.make_async_copy(w_query, wq, local_sem.at[2]),
        pltpu.make_async_copy(w_value, wv, local_sem.at[3]),
        pltpu.make_async_copy(w_out, wo.at[0], local_sem.at[4]),
    ]
    for copy in local[:4]:
        copy.start()

    barrier = pltpu.get_barrier_semaphore()
    pl.semaphore_signal(barrier, inc=1, device_id={"tp": other})
    pl.semaphore_signal(barrier, inc=1, device_id={"sp": mate})

    @pl.when(has_up)
    def _():
        pl.semaphore_signal(barrier, inc=1, device_id={"sp": me + 2})

    @pl.when(has_down)
    def _():
        pl.semaphore_signal(barrier, inc=1, device_id={"sp": me - 2})

    half_rows = lax.broadcasted_iota(jnp.int32, (half, half), 0)
    half_cols = lax.broadcasted_iota(jnp.int32, (half, half), 1)
    half_bits = per_half.bit_length() - 1
    half_time = classes * (half_rows & (per_half - 1)) + (half_rows >> half_bits)
    half_perm[...] = (half_time == half_cols).astype(F32).astype(BF16)

    local[0].wait()
    x[:, core] = (
        jnp.dot(half_perm[...], xin[...], preferred_element_type=F32)
        .astype(BF16)
        .reshape(classes, per_half, depth)
    )
    peers = 2 + jnp.where(has_up, 1, 0) + jnp.where(has_down, 1, 0)
    pl.semaphore_wait(barrier, peers)
    x_copy = pltpu.make_async_remote_copy(
        src_ref=x.at[:, core],
        dst_ref=x.at[:, core],
        send_sem=x_send,
        recv_sem=x_recv,
        device_id={"tp": other},
    )
    x_copy.start()
    my_rows = pl.ds(pl.multiple_of(core * half, half), half)
    their_rows = pl.ds(pl.multiple_of(other * half, half), half)

    def project(weights, side):
        rows = x[:, side].reshape(half, depth)
        return jnp.dot(rows, weights[...], preferred_element_type=F32)

    def place_keys(side):
        keys = project(wk, side).astype(BF16)
        for c in range(n_chunks):
            piece = keys[:, c * LANES : (c + 1) * LANES]
            kbuf[0, c, :, side] = piece.reshape(classes, per_half, LANES)

    def place_queries(side):
        queries = (project(wq, side) * HEAD_DIM**-0.5).astype(BF16)
        nat[0, :, side] = queries.reshape(classes, per_half, queries.shape[1])

    def place_values(side):
        values = project(wv, side).astype(BF16)
        nat[1, :, side] = values.reshape(classes, per_half, values.shape[1])

    def key_copy(c, late):
        side = core + late * (1 - 2 * core)
        return pltpu.make_async_remote_copy(
            src_ref=kbuf.at[0, c, :, side],
            dst_ref=kbuf.at[1, c, :, side],
            send_sem=kv_send.at[c, late],
            recv_sem=kv_recv.at[c, late],
            device_id={"sp": mate},
        )

    def value_copy(c):
        return pltpu.make_async_remote_copy(
            src_ref=vbuf.at[0, c],
            dst_ref=vbuf.at[1, c],
            send_sem=kv_send.at[c, 2],
            recv_sem=kv_recv.at[c, 2],
            device_id={"sp": mate},
        )

    def query_copy(s, relay):
        return pltpu.make_async_remote_copy(
            src_ref=qbuf.at[relay, s],
            dst_ref=qbuf.at[relay + 1, s],
            send_sem=q_send.at[relay, s],
            recv_sem=q_recv.at[relay, s],
            device_id={"sp": down},
        )

    def out_copies(kind, s):
        return [
            pltpu.make_async_remote_copy(
                src_ref=src.at[kind, s],
                dst_ref=dst.at[kind, s],
                send_sem=o_send.at[kind, s, i],
                recv_sem=o_recv.at[kind, s, i],
                device_id={"sp": up},
            )
            for i, (src, dst) in enumerate(((o_out, o_in), (s_out, s_in)))
        ]

    def hidden_copy(c):
        return pltpu.make_async_remote_copy(
            src_ref=hid_nat.at[c, their_rows],
            dst_ref=hid_in.at[c],
            send_sem=h_send.at[c],
            recv_sem=h_recv.at[c],
            device_id={"tp": other},
        )

    w_copy = pltpu.make_async_remote_copy(
        src_ref=w_out,
        dst_ref=wo.at[1],
        send_sem=w_send,
        recv_sem=w_recv,
        device_id={"tp": other},
    )

    def turned(which, c):
        lanes = slice(c * LANES, (c + 1) * LANES)
        return nat[which].reshape(length, n_chunks * LANES)[:, lanes].T

    local[1].wait()
    place_keys(core)
    early = n_chunks // 2
    for c in range(early):
        key_copy(c, 0).start()
    local[2].wait()
    place_queries(core)
    local[3].wait()
    local[4].start()
    place_values(core)

    x_copy.wait()
    place_queries(other)
    groups = 2
    wide = length // groups
    for c in range(n_chunks):
        queries = turned(0, c)
        for g in range(groups):
            qbuf[0, c * groups + g] = queries[:, g * wide : (g + 1) * wide]
            if c == 0:

                @pl.when(has_down)
                def _():
                    query_copy(g, 0).start()

    place_keys(other)
    key_copy(0, 1).start()
    place_values(other)
    for c in range(n_chunks):
        if c >= early:
            key_copy(c, 0).start()
        if c >= 1:
            key_copy(c, 1).start()
        vbuf[0, c] = turned(1, c)
        value_copy(c).start()
    w_copy.start()

    key_step = lax.broadcasted_iota(jnp.int32, (per, per), 0)
    query_step = lax.broadcasted_iota(jnp.int32, (per, per), 1)
    tail = per // classes
    tail_bits = tail.bit_length() - 1
    heads_per = LANES // HEAD_DIM

    def slope_of(head):
        number = core * (n_chunks * heads_per) + head + 1
        exponent = jnp.full((1, per), number, jnp.int32).astype(F32)
        return jnp.exp2(exponent * (-ALIBI_EXP / HEADS))

    slopes = [slope_of(h) for h in range(n_chunks * heads_per)]

    def fill(first_row, distance, logc):
        gap = distance.astype(F32)
        rows = pl.ds(pl.multiple_of(first_row, per), per)
        for h in range(n_chunks * heads_per):
            c, j = divmod(h, heads_per)
            tab[c, rows, j * per : (j + 1) * per] = logc - slopes[h] * gap

    steps = classes * (query_step - key_step)
    T0 = 0
    T_CLASS = (2 * classes - 1) * per
    T_TAIL = T_CLASS + classes * per

    @pl.loop(0, 2 * classes - 1)
    def _(e):
        distance = steps + (classes - 1 - e)
        fill(T0 + e * per, distance, log_multiplicity(distance))

    @pl.loop(0, classes)
    def _(e):
        distance = steps + (e + 1) * length
        fill(T_CLASS + e * per, distance, log_multiplicity(distance))

    tail_class = key_step >> tail_bits
    tail_step = (key_step & (tail - 1)) + (per - tail)

    @pl.loop(0, classes)
    def _(r):
        distance = length + classes * (query_step - tail_step) + (r - tail_class)
        logc = jnp.where(tail_class == r, -jnp.inf, log_multiplicity(distance))
        fill(T_TAIL + r * per, distance, logc)

    rows = lax.broadcasted_iota(jnp.int32, (length, length), 0)
    cols = lax.broadcasted_iota(jnp.int32, (length, length), 1)
    per_bits = per.bit_length() - 1
    time_of_row = classes * (rows & (per - 1)) + (rows >> per_bits)
    back_perm[...] = (time_of_row == cols).astype(F32).astype(BF16)
    pick_rows = lax.broadcasted_iota(jnp.int32, (length, per), 0)
    pick_cols = lax.broadcasted_iota(jnp.int32, (length, per), 1)
    pick = (pick_cols >> tail_bits) * per + (per - tail) + (pick_cols & (tail - 1))
    tail_pick[...] = (pick_rows == pick).astype(F32).astype(BF16)

    ones_of = functools.partial(jnp.ones, dtype=BF16)

    def class_part(slot, c, r, table):
        keys = kbuf[slot, c, r].reshape(per, LANES)
        bias = tab[c, table : table + per, :]
        return keys, bias, vbuf[slot, c, :, r * per : (r + 1) * per]

    def gap_table(blocks):
        return T_CLASS + (blocks - 1) * per

    def tail_part(c, r):
        keys = jnp.concatenate(
            [kbuf[1, c, k, 1, per_half - tail :, :] for k in range(classes)], axis=0
        )
        table = T_TAIL + r * per
        return keys, tab[c, table : table + per, :], vtail[c]

    def own_part(c, r):
        first = T0 + (classes - 1 - r) * per
        return (
            kbuf[0, c].reshape(length, LANES),
            tab[c, first : first + length, :],
            vbuf[0, c],
        )

    per_group = classes // groups

    def score(c, g, i, q_slot, parts_of):
        piece = c * groups + g
        lanes = slice(i * per, (i + 1) * per)
        parts = parts_of(g * per_group + i)
        first = qbuf[q_slot, piece, :HEAD_DIM, lanes]
        second = qbuf[q_slot, piece, HEAD_DIM:, lanes]
        blank = jnp.zeros_like(first)
        queries = jnp.concatenate(
            [
                jnp.concatenate([first, blank], axis=0),
                jnp.concatenate([blank, second], axis=0),
            ],
            axis=1,
        )
        scores = [
            jnp.dot(keys, queries, preferred_element_type=F32) + bias
            for keys, bias, _ in parts
        ]
        tops = [jnp.max(s, axis=0, keepdims=True) for s in scores]
        values = jnp.concatenate([v for _, _, v in parts], axis=1)
        return scores, functools.reduce(jnp.maximum, tops), values

    def weigh(item, c, g, i, scores, top, values):
        piece = c * groups + g
        lanes = slice(i * per, (i + 1) * per)
        weights = jnp.concatenate(
            [jnp.exp(s - top).astype(BF16) for s in scores], axis=0
        )
        count = values.shape[1]
        for j in range(heads_per):
            mine = values[j * HEAD_DIM : (j + 1) * HEAD_DIM]
            summed = jnp.dot(
                jnp.concatenate([mine, ones_of((ONES, count))], axis=0),
                weights[:, j * per : (j + 1) * per],
                preferred_element_type=F32,
            )
            row = slice(i * heads_per + j, i * heads_per + j + 1)
            acc[item, piece, j * HEAD_DIM : (j + 1) * HEAD_DIM, lanes] = summed[:HEAD_DIM]
            l_ref[item, piece, row, :] = summed[HEAD_DIM : HEAD_DIM + 1]
            m_ref[item, piece, row, :] = top[:, j * per : (j + 1) * per]

    def attend(c, g, items):
        held = None
        for i in range(per_group):
            for item, q_slot, parts_of in items:
                scored = (item, c, g, i, *score(c, g, i, q_slot, parts_of))
                if held is not None:
                    weigh(*held)
                held = scored
        weigh(*held)

    def blocks():
        for i in range(per_group):
            for j in range(heads_per):
                row = slice(i * heads_per + j, i * heads_per + j + 1)
                dims = slice(j * HEAD_DIM, (j + 1) * HEAD_DIM)
                yield row, dims, slice(i * per, (i + 1) * per)

    def take_in(item, s, kind):
        for copy in out_copies(kind, s):
            copy.wait_recv()
        here, there = m_ref[item, s], s_in[kind, s]
        top = jnp.maximum(here, there)
        keep, gain = jnp.exp(here - top), jnp.exp(there - top)
        m_ref[item, s] = top
        l_ref[item, s] = keep * l_ref[item, s] + gain
        for row, dims, lanes in blocks():
            acc[item, s, dims, lanes] = (
                keep[row] * acc[item, s, dims, lanes]
                + gain[row] * o_in[kind, s, dims, lanes].astype(F32)
            )

    def level(item, s, out):
        total = l_ref[item, s]
        scale = 1.0 / total
        for row, dims, lanes in blocks():
            out[dims, lanes] = (acc[item, s, dims, lanes] * scale[row]).astype(BF16)
        return m_ref[item, s] + jnp.log(total)

    def emit(item, s):
        s_out[item, s] = level(item, s, o_out.at[item, s])
        for copy in out_copies(item, s):
            copy.start()

    def finish(c, g):
        piece = c * groups + g

        @pl.when(has_down)
        def _():
            take_in(OWN, piece, UP)

        logs[piece] = level(OWN, piece, hid.at[c, :, g * wide : (g + 1) * wide])
        if g == groups - 1:
            hid_nat[c] = (
                jnp.dot(hid[c], back_perm[...], preferred_element_type=F32).astype(BF16).T
            )
            hidden_copy(c).start()

    n_pieces = n_chunks * groups

    def merge_up(s):
        @pl.when(has_up & (s >= 0) & (s < n_pieces))
        def _():
            @pl.when(has_down)
            def _():
                take_in(UP, s, FAR)

            emit(UP, s)

    def pass_on(s):
        @pl.when(has_up & (s < n_pieces))
        def _():
            query_copy(s, 0).wait_recv()

            @pl.when(has_down)
            def _():
                query_copy(s, 1).start()

        @pl.when(has_down & (s + groups < n_pieces))
        def _():
            query_copy(s + groups, 0).start()

    def attend_all(c, g):
        if g == 0:
            key_copy(c, 0).wait_recv()
            key_copy(c, 1).wait_recv()
            value_copy(c).wait_recv()
            vtail[c] = jnp.dot(
                vbuf[1, c], tail_pick[...], preferred_element_type=F32
            ).astype(BF16)

        piece = c * groups + g

        @pl.when(has_far)
        def _():
            query_copy(piece, 1).wait_recv()

            @pl.when(is_even)
            def _():
                attend(
                    c,
                    g,
                    [
                        (
                            FAR,
                            2,
                            lambda r: [
                                class_part(0, c, r, gap_table(4)),
                                class_part(1, c, r, gap_table(3)),
                            ],
                        ),
                    ],
                )

            @pl.when(is_odd)
            def _():
                attend(c, g, [(FAR, 2, lambda r: [class_part(0, c, r, gap_table(4))])])

            emit(FAR, piece)

        @pl.when(is_even)
        def _():
            attend(
                c,
                g,
                [
                    (
                        UP,
                        1,
                        lambda r: [
                            class_part(0, c, r, gap_table(2)),
                            class_part(1, c, r, gap_table(1)),
                            tail_part(c, r),
                        ],
                    ),
                    (OWN, 0, lambda r: [own_part(c, r)]),
                ],
            )

        @pl.when(is_odd)
        def _():
            attend(
                c,
                g,
                [
                    (
                        UP,
                        1,
                        lambda r: [
                            class_part(0, c, r, gap_table(2)),
                            class_part(1, c, r, gap_table(3)),
                        ],
                    ),
                    (
                        OWN,
                        0,
                        lambda r: [
                            own_part(c, r),
                            class_part(1, c, r, gap_table(1)),
                            tail_part(c, r),
                        ],
                    ),
                ],
            )

    @pl.loop(0, n_chunks + 1)
    def _(c):
        for g in range(groups):
            beat = c * groups + g
            pass_on(beat)
            merge_up(beat - 3)
            if g == 0:

                @pl.when(c >= 1)
                def _():
                    attend_all(c - 1, groups - 1)

            else:

                @pl.when(c < n_chunks)
                def _():
                    attend_all(c, g - 1)

            @pl.when(c >= 2)
            def _():
                finish(c - 2, g)

    out_width = wo.shape[2]
    n_parts = max(1, out_width // 512)
    part_width = out_width // n_parts
    done = n_chunks - 1

    def all_parts():
        return [slice(p * part_width, (p + 1) * part_width) for p in range(n_parts)]

    def spread(first, last_):
        return jnp.concatenate(
            [hid_nat[c, my_rows, :] for c in range(first, last_)]
            + [hid_in[c] for c in range(first, last_)],
            axis=1,
        )

    def weights_of(first, last_, lanes):
        rows_ = slice(first * LANES, last_ * LANES)
        return jnp.concatenate([wo[0, rows_, lanes], wo[1, rows_, lanes]], axis=0)

    merge_up(n_pieces - 1)
    local[4].wait()
    w_copy.wait()
    for c in range(done):
        hidden_copy(c).wait_recv()
    sofar = spread(0, done)
    for lanes in all_parts():
        part_sum[:, lanes] = jnp.dot(
            sofar, weights_of(0, done, lanes), preferred_element_type=F32
        )
    for g in range(groups):
        finish(done, g)

    ordered = jnp.concatenate(
        [
            jnp.concatenate(
                [
                    logs[c * groups + g, i * heads_per + j : i * heads_per + j + 1, :]
                    for g in range(groups)
                    for i in range(per_group)
                ],
                axis=1,
            )
            for c in range(n_chunks)
            for j in range(heads_per)
        ],
        axis=0,
    )
    high = ordered.astype(BF16)
    left = ordered - high.astype(F32)
    middle = left.astype(BF16)
    low = (left - middle.astype(F32)).astype(BF16)
    log_sums[...] = functools.reduce(
        jnp.add,
        [
            jnp.dot(piece, back_perm[...], preferred_element_type=F32)
            for piece in (low, middle, high)
        ],
    )
    for c in range(done, n_chunks):
        hidden_copy(c).wait_recv()
    late = spread(done, n_chunks)
    for lanes in all_parts():
        rest = jnp.dot(late, weights_of(done, n_chunks, lanes), preferred_element_type=F32)
        mixed[:, lanes] = (part_sum[:, lanes] + rest).astype(BF16)

    @pl.loop(0, n_chunks)
    def _(c):
        key_copy(c, 0).wait_send()
        key_copy(c, 1).wait_send()
        value_copy(c).wait_send()
        hidden_copy(c).wait_send()

    @pl.loop(0, n_pieces)
    def _(s):
        @pl.when(has_down)
        def _():
            query_copy(s, 0).wait_send()

        @pl.when(has_down & has_up)
        def _():
            query_copy(s, 1).wait_send()

        @pl.when(has_far)
        def _():
            for copy in out_copies(FAR, s):
                copy.wait_send()

        @pl.when(has_up)
        def _():
            for copy in out_copies(UP, s):
                copy.wait_send()


def body(n_sp, tokens, w_query, w_key, w_value, w_out):
    half, depth = tokens.shape
    length = 2 * half
    width = w_query.shape[1]
    out_width = w_out.shape[1]
    heads = width // HEAD_DIM
    chunks = width // LANES
    assert REACH == MIDDLE_DILATION * length and n_sp % 2 == 0
    per = length // MIDDLE_DILATION
    groups = 2
    pieces, wide = chunks * groups, length // groups
    stats = MIDDLE_DILATION // groups * (LANES // HEAD_DIM)
    tables = (4 * MIDDLE_DILATION - 1) * per
    hbm = pl.BlockSpec(memory_space=pl.ANY)
    vmem = pl.BlockSpec(memory_space=pltpu.VMEM)
    dma = pltpu.SemaphoreType.DMA
    return pl.pallas_call(
        functools.partial(kernel, n_sp),
        out_shape=(
            jax.ShapeDtypeStruct((half, out_width), BF16),
            jax.ShapeDtypeStruct((heads, length), F32),
        ),
        in_specs=[hbm] * 5,
        out_specs=(vmem, vmem),
        scratch_shapes=[
            pltpu.VMEM((half, depth), BF16),
            pltpu.VMEM((MIDDLE_DILATION, 2, per // 2, depth), BF16),
            pltpu.VMEM((depth, width), BF16),
            pltpu.VMEM((depth, width), BF16),
            pltpu.VMEM((depth, width), BF16),
            pltpu.VMEM((2, width, out_width), BF16),
            pltpu.VMEM((2, MIDDLE_DILATION, 2, per // 2, width), BF16),
            pltpu.VMEM((2, chunks, MIDDLE_DILATION, 2, per // 2, LANES), BF16),
            pltpu.VMEM((2, chunks, LANES, length), BF16),
            pltpu.VMEM((chunks, LANES, per), BF16),
            pltpu.VMEM((3, pieces, LANES, wide), BF16),
            pltpu.VMEM((half, half), BF16),
            pltpu.VMEM((length, length), BF16),
            pltpu.VMEM((length, per), BF16),
            pltpu.VMEM((chunks, tables, 2 * per), F32),
            pltpu.VMEM((3, pieces, stats, per), F32),
            pltpu.VMEM((3, pieces, stats, per), F32),
            pltpu.VMEM((3, pieces, LANES, wide), F32),
            pltpu.VMEM((2, pieces, LANES, wide), BF16),
            pltpu.VMEM((2, pieces, stats, per), F32),
            pltpu.VMEM((2, pieces, LANES, wide), BF16),
            pltpu.VMEM((2, pieces, stats, per), F32),
            pltpu.VMEM((chunks, LANES, length), BF16),
            pltpu.VMEM((chunks, length, LANES), BF16),
            pltpu.VMEM((pieces, stats, per), F32),
            pltpu.VMEM((chunks, half, LANES), BF16),
            pltpu.VMEM((half, out_width), F32),
            dma((5,)),
            dma,
            dma,
            dma((chunks, 3)),
            dma((chunks, 3)),
            dma((2, pieces)),
            dma((2, pieces)),
            dma((2, pieces, 2)),
            dma((2, pieces, 2)),
            dma((chunks,)),
            dma((chunks,)),
            dma,
            dma,
        ],
        compiler_params=pltpu.CompilerParams(
            collective_id=0, has_side_effects=True, vmem_limit_bytes=52 * 1024 * 1024
        ),
        name="dilated_layer",
    )(tokens, w_query, w_key, w_value, w_out)


def solution(mesh):
    in_specs = (
        P(("grp", "sp", "tp"), None),
        P(None, "tp"),
        P(None, "tp"),
        P(None, "tp"),
        P("tp", None),
    )
    out_specs = (P(("grp", "sp", "tp"), None), P("tp", ("grp", "sp")))
    return jax.shard_map(
        functools.partial(body, mesh.shape["sp"]),
        mesh=mesh,
        in_specs=in_specs,
        out_specs=out_specs,
        check_vma=False,
    )
```

```python
import functools
import math

import jax
import jax.numpy as jnp
from jax import lax
from jax.experimental import pallas as pl
from jax.experimental.pallas import tpu as pltpu
from jax.sharding import PartitionSpec as P

HEADS = 16
HEAD_DIM = 64
WINDOW_KEY_STEPS = 128
MIDDLE_DILATION = 4
FAR_DILATION = 16
REACH = 2048
ALIBI_EXP = 16.0
LANES = 128
ONES = 16
F32 = jnp.float32
BF16 = jnp.bfloat16
FAR, UP, OWN = 0, 1, 2


def log_multiplicity(distance):
    def window(stride):
        inside = (distance >= 0) & (distance <= WINDOW_KEY_STEPS * stride)
        if stride > 1:
            inside = inside & ((distance & (stride - 1)) == 0)
        return inside.astype(jnp.int32)

    count = window(1) + window(MIDDLE_DILATION) + window(FAR_DILATION)
    return jnp.where(
        count == 3,
        math.log(3.0),
        jnp.where(count == 2, math.log(2.0), jnp.where(count == 1, 0.0, -jnp.inf)),
    ).astype(F32)


def kernel(
    n_sp,
    tokens,
    w_query,
    w_key,
    w_value,
    w_out,
    mixed,
    log_sums,
    xin,
    x,
    wq,
    wk,
    wv,
    wo,
    nat,
    kbuf,
    vbuf,
    vtail,
    qbuf,
    half_perm,
    back_perm,
    tail_pick,
    tab,
    m_ref,
    l_ref,
    acc,
    o_out,
    s_out,
    o_in,
    s_in,
    hid,
    hid_nat,
    logs,
    hid_in,
    part_sum,
    local_sem,
    x_send,
    x_recv,
    kv_send,
    kv_recv,
    q_send,
    q_recv,
    o_send,
    o_recv,
    h_send,
    h_recv,
    w_send,
    w_recv,
):
    half, depth = tokens.shape
    length = 2 * half
    n_chunks = kbuf.shape[1]
    classes = MIDDLE_DILATION
    per = length // classes
    per_half = per // 2
    me = lax.axis_index("sp")
    core = lax.axis_index("tp")
    other = 1 - core
    odd = lax.rem(me, 2)
    mate = me + 1 - 2 * odd
    is_even = odd == 0
    is_odd = odd == 1
    has_up = me + 2 < n_sp
    has_far = me + 4 < n_sp
    has_down = me >= 2
    up = jnp.where(has_up, me + 2, me - 2)
    down = jnp.where(has_down, me - 2, me + 2)

    local = [
        pltpu.make_async_copy(tokens, xin, local_sem.at[0]),
        pltpu.make_async_copy(w_key, wk, local_sem.at[1]),
        pltpu.make_async_copy(w_query, wq, local_sem.at[2]),
        pltpu.make_async_copy(w_value, wv, local_sem.at[3]),
        pltpu.make_async_copy(w_out, wo.at[0], local_sem.at[4]),
    ]
    for copy in local[:4]:
        copy.start()

    barrier = pltpu.get_barrier_semaphore()
    pl.semaphore_signal(barrier, inc=1, device_id={"tp": other})
    pl.semaphore_signal(barrier, inc=1, device_id={"sp": mate})

    @pl.when(has_up)
    def _():
        pl.semaphore_signal(barrier, inc=1, device_id={"sp": me + 2})

    @pl.when(has_down)
    def _():
        pl.semaphore_signal(barrier, inc=1, device_id={"sp": me - 2})

    half_rows = lax.broadcasted_iota(jnp.int32, (half, half), 0)
    half_cols = lax.broadcasted_iota(jnp.int32, (half, half), 1)
    half_bits = per_half.bit_length() - 1
    half_time = classes * (half_rows & (per_half - 1)) + (half_rows >> half_bits)
    half_perm[...] = (half_time == half_cols).astype(F32).astype(BF16)

    local[0].wait()
    x[:, core] = (
        jnp.dot(half_perm[...], xin[...], preferred_element_type=F32)
        .astype(BF16)
        .reshape(classes, per_half, depth)
    )
    peers = 2 + jnp.where(has_up, 1, 0) + jnp.where(has_down, 1, 0)
    pl.semaphore_wait(barrier, peers)
    x_copy = pltpu.make_async_remote_copy(
        src_ref=x.at[:, core],
        dst_ref=x.at[:, core],
        send_sem=x_send,
        recv_sem=x_recv,
        device_id={"tp": other},
    )
    x_copy.start()
    my_rows = pl.ds(pl.multiple_of(core * half, half), half)
    their_rows = pl.ds(pl.multiple_of(other * half, half), half)

    def project(weights, side):
        rows = x[:, side].reshape(half, depth)
        return jnp.dot(rows, weights[...], preferred_element_type=F32)

    def place_keys(side):
        keys = project(wk, side).astype(BF16)
        for c in range(n_chunks):
            piece = keys[:, c * LANES : (c + 1) * LANES]
            kbuf[0, c, :, side] = piece.reshape(classes, per_half, LANES)

    def place_queries(side):
        queries = (project(wq, side) * HEAD_DIM**-0.5).astype(BF16)
        nat[0, :, side] = queries.reshape(classes, per_half, queries.shape[1])

    def place_values(side):
        values = project(wv, side).astype(BF16)
        nat[1, :, side] = values.reshape(classes, per_half, values.shape[1])

    def key_copy(c, late):
        side = core + late * (1 - 2 * core)
        return pltpu.make_async_remote_copy(
            src_ref=kbuf.at[0, c, :, side],
            dst_ref=kbuf.at[1, c, :, side],
            send_sem=kv_send.at[c, late],
            recv_sem=kv_recv.at[c, late],
            device_id={"sp": mate},
        )

    def value_copy(c):
        return pltpu.make_async_remote_copy(
            src_ref=vbuf.at[0, c],
            dst_ref=vbuf.at[1, c],
            send_sem=kv_send.at[c, 2],
            recv_sem=kv_recv.at[c, 2],
            device_id={"sp": mate},
        )

    def query_copy(s, relay):
        return pltpu.make_async_remote_copy(
            src_ref=qbuf.at[relay, s],
            dst_ref=qbuf.at[relay + 1, s],
            send_sem=q_send.at[relay, s],
            recv_sem=q_recv.at[relay, s],
            device_id={"sp": down},
        )

    def out_copies(kind, s):
        return [
            pltpu.make_async_remote_copy(
                src_ref=src.at[kind, s],
                dst_ref=dst.at[kind, s],
                send_sem=o_send.at[kind, s, i],
                recv_sem=o_recv.at[kind, s, i],
                device_id={"sp": up},
            )
            for i, (src, dst) in enumerate(((o_out, o_in), (s_out, s_in)))
        ]

    def hidden_copy(c):
        return pltpu.make_async_remote_copy(
            src_ref=hid_nat.at[c, their_rows],
            dst_ref=hid_in.at[c],
            send_sem=h_send.at[c],
            recv_sem=h_recv.at[c],
            device_id={"tp": other},
        )

    w_copy = pltpu.make_async_remote_copy(
        src_ref=w_out,
        dst_ref=wo.at[1],
        send_sem=w_send,
        recv_sem=w_recv,
        device_id={"tp": other},
    )

    def turned(which, c):
        lanes = slice(c * LANES, (c + 1) * LANES)
        return nat[which].reshape(length, n_chunks * LANES)[:, lanes].T

    local[1].wait()
    place_keys(core)
    early = n_chunks // 2
    for c in range(early):
        key_copy(c, 0).start()
    local[2].wait()
    place_queries(core)
    local[3].wait()
    local[4].start()
    place_values(core)

    x_copy.wait()
    place_queries(other)
    groups = 2
    wide = length // groups
    for c in range(n_chunks):
        queries = turned(0, c)
        for g in range(groups):
            qbuf[0, c * groups + g] = queries[:, g * wide : (g + 1) * wide]
            if c == 0:

                @pl.when(has_down)
                def _():
                    query_copy(g, 0).start()

    place_keys(other)
    key_copy(0, 1).start()
    place_values(other)
    for c in range(n_chunks):
        if c >= early:
            key_copy(c, 0).start()
        if c >= 1:
            key_copy(c, 1).start()
        vbuf[0, c] = turned(1, c)
        value_copy(c).start()

    key_step = lax.broadcasted_iota(jnp.int32, (per, per), 0)
    query_step = lax.broadcasted_iota(jnp.int32, (per, per), 1)
    tail = per // classes
    tail_bits = tail.bit_length() - 1
    heads_per = LANES // HEAD_DIM

    def slope_of(head):
        number = core * (n_chunks * heads_per) + head + 1
        exponent = jnp.full((1, per), number, jnp.int32).astype(F32)
        return jnp.exp2(exponent * (-ALIBI_EXP / HEADS))

    slopes = [slope_of(h) for h in range(n_chunks * heads_per)]

    def fill(first_row, distance, logc):
        gap = distance.astype(F32)
        rows = pl.ds(pl.multiple_of(first_row, per), per)
        for h in range(n_chunks * heads_per):
            c, j = divmod(h, heads_per)
            tab[c, rows, j * per : (j + 1) * per] = logc - slopes[h] * gap

    steps = classes * (query_step - key_step)
    T0 = 0
    T_CLASS = (2 * classes - 1) * per
    T_TAIL = T_CLASS + classes * per

    @pl.loop(0, 2 * classes - 1)
    def _(e):
        distance = steps + (classes - 1 - e)
        fill(T0 + e * per, distance, log_multiplicity(distance))

    @pl.loop(0, classes)
    def _(e):
        distance = steps + (e + 1) * length
        fill(T_CLASS + e * per, distance, log_multiplicity(distance))

    tail_class = key_step >> tail_bits
    tail_step = (key_step & (tail - 1)) + (per - tail)

    @pl.loop(0, classes)
    def _(r):
        distance = length + classes * (query_step - tail_step) + (r - tail_class)
        logc = jnp.where(tail_class == r, -jnp.inf, log_multiplicity(distance))
        fill(T_TAIL + r * per, distance, logc)

    rows = lax.broadcasted_iota(jnp.int32, (length, length), 0)
    cols = lax.broadcasted_iota(jnp.int32, (length, length), 1)
    per_bits = per.bit_length() - 1
    time_of_row = classes * (rows & (per - 1)) + (rows >> per_bits)
    back_perm[...] = (time_of_row == cols).astype(F32).astype(BF16)
    pick_rows = lax.broadcasted_iota(jnp.int32, (length, per), 0)
    pick_cols = lax.broadcasted_iota(jnp.int32, (length, per), 1)
    pick = (pick_cols >> tail_bits) * per + (per - tail) + (pick_cols & (tail - 1))
    tail_pick[...] = (pick_rows == pick).astype(F32).astype(BF16)

    ones_of = functools.partial(jnp.ones, dtype=BF16)

    def class_part(slot, c, r, table):
        keys = kbuf[slot, c, r].reshape(per, LANES)
        bias = tab[c, table : table + per, :]
        return keys, bias, vbuf[slot, c, :, r * per : (r + 1) * per]

    def gap_table(blocks):
        return T_CLASS + (blocks - 1) * per

    def tail_part(c, r):
        keys = jnp.concatenate(
            [kbuf[1, c, k, 1, per_half - tail :, :] for k in range(classes)], axis=0
        )
        table = T_TAIL + r * per
        return keys, tab[c, table : table + per, :], vtail[c]

    def own_part(c, r):
        first = T0 + (classes - 1 - r) * per
        return (
            kbuf[0, c].reshape(length, LANES),
            tab[c, first : first + length, :],
            vbuf[0, c],
        )

    per_group = classes // groups

    def score(c, g, i, q_slot, parts_of):
        piece = c * groups + g
        lanes = slice(i * per, (i + 1) * per)
        parts = parts_of(g * per_group + i)
        first = qbuf[q_slot, piece, :HEAD_DIM, lanes]
        second = qbuf[q_slot, piece, HEAD_DIM:, lanes]
        blank = jnp.zeros_like(first)
        queries = jnp.concatenate(
            [
                jnp.concatenate([first, blank], axis=0),
                jnp.concatenate([blank, second], axis=0),
            ],
            axis=1,
        )
        scores = [
            jnp.dot(keys, queries, preferred_element_type=F32) + bias
            for keys, bias, _ in parts
        ]
        tops = [jnp.max(s, axis=0, keepdims=True) for s in scores]
        values = jnp.concatenate([v for _, _, v in parts], axis=1)
        return scores, functools.reduce(jnp.maximum, tops), values

    def weigh(item, c, g, i, scores, top, values):
        piece = c * groups + g
        lanes = slice(i * per, (i + 1) * per)
        weights = jnp.concatenate(
            [jnp.exp(s - top).astype(BF16) for s in scores], axis=0
        )
        count = values.shape[1]
        for j in range(heads_per):
            mine = values[j * HEAD_DIM : (j + 1) * HEAD_DIM]
            summed = jnp.dot(
                jnp.concatenate([mine, ones_of((ONES, count))], axis=0),
                weights[:, j * per : (j + 1) * per],
                preferred_element_type=F32,
            )
            row = slice(i * heads_per + j, i * heads_per + j + 1)
            acc[item, piece, j * HEAD_DIM : (j + 1) * HEAD_DIM, lanes] = summed[:HEAD_DIM]
            l_ref[item, piece, row, :] = summed[HEAD_DIM : HEAD_DIM + 1]
            m_ref[item, piece, row, :] = top[:, j * per : (j + 1) * per]

    def attend(c, g, items):
        held = None
        for i in range(per_group):
            for item, q_slot, parts_of in items:
                scored = (item, c, g, i, *score(c, g, i, q_slot, parts_of))
                if held is not None:
                    weigh(*held)
                held = scored
        weigh(*held)

    def blocks():
        for i in range(per_group):
            for j in range(heads_per):
                row = slice(i * heads_per + j, i * heads_per + j + 1)
                dims = slice(j * HEAD_DIM, (j + 1) * HEAD_DIM)
                yield row, dims, slice(i * per, (i + 1) * per)

    def take_in(item, s, kind):
        for copy in out_copies(kind, s):
            copy.wait_recv()
        here, there = m_ref[item, s], s_in[kind, s]
        top = jnp.maximum(here, there)
        keep, gain = jnp.exp(here - top), jnp.exp(there - top)
        m_ref[item, s] = top
        l_ref[item, s] = keep * l_ref[item, s] + gain
        for row, dims, lanes in blocks():
            acc[item, s, dims, lanes] = (
                keep[row] * acc[item, s, dims, lanes]
                + gain[row] * o_in[kind, s, dims, lanes].astype(F32)
            )

    def level(item, s, out):
        total = l_ref[item, s]
        scale = 1.0 / total
        for row, dims, lanes in blocks():
            out[dims, lanes] = (acc[item, s, dims, lanes] * scale[row]).astype(BF16)
        return m_ref[item, s] + jnp.log(total)

    def emit(item, s):
        s_out[item, s] = level(item, s, o_out.at[item, s])
        for copy in out_copies(item, s):
            copy.start()

    def finish(c, g):
        piece = c * groups + g

        @pl.when(has_down)
        def _():
            take_in(OWN, piece, UP)

        logs[piece] = level(OWN, piece, hid.at[c, :, g * wide : (g + 1) * wide])
        if g == groups - 1:
            hid_nat[c] = (
                jnp.dot(hid[c], back_perm[...], preferred_element_type=F32).astype(BF16).T
            )
            hidden_copy(c).start()

    n_pieces = n_chunks * groups

    def merge_up(s):
        @pl.when(has_up & (s >= 0) & (s < n_pieces))
        def _():
            @pl.when(has_down)
            def _():
                take_in(UP, s, FAR)

            emit(UP, s)

    def pass_on(s):
        @pl.when(has_up & (s < n_pieces))
        def _():
            query_copy(s, 0).wait_recv()

            @pl.when(has_down)
            def _():
                query_copy(s, 1).start()

        @pl.when(has_down & (s + groups < n_pieces))
        def _():
            query_copy(s + groups, 0).start()

    def attend_all(c, g):
        if g == 0:
            key_copy(c, 0).wait_recv()
            key_copy(c, 1).wait_recv()
            value_copy(c).wait_recv()
            vtail[c] = jnp.dot(
                vbuf[1, c], tail_pick[...], preferred_element_type=F32
            ).astype(BF16)

        piece = c * groups + g

        @pl.when(has_far)
        def _():
            query_copy(piece, 1).wait_recv()

            @pl.when(is_even)
            def _():
                attend(
                    c,
                    g,
                    [
                        (
                            FAR,
                            2,
                            lambda r: [
                                class_part(0, c, r, gap_table(4)),
                                class_part(1, c, r, gap_table(3)),
                            ],
                        ),
                    ],
                )

            @pl.when(is_odd)
            def _():
                attend(c, g, [(FAR, 2, lambda r: [class_part(0, c, r, gap_table(4))])])

            emit(FAR, piece)

        @pl.when(is_even)
        def _():
            attend(
                c,
                g,
                [
                    (
                        UP,
                        1,
                        lambda r: [
                            class_part(0, c, r, gap_table(2)),
                            class_part(1, c, r, gap_table(1)),
                            tail_part(c, r),
                        ],
                    ),
                    (OWN, 0, lambda r: [own_part(c, r)]),
                ],
            )

        @pl.when(is_odd)
        def _():
            attend(
                c,
                g,
                [
                    (
                        UP,
                        1,
                        lambda r: [
                            class_part(0, c, r, gap_table(2)),
                            class_part(1, c, r, gap_table(3)),
                        ],
                    ),
                    (
                        OWN,
                        0,
                        lambda r: [
                            own_part(c, r),
                            class_part(1, c, r, gap_table(1)),
                            tail_part(c, r),
                        ],
                    ),
                ],
            )

    @pl.loop(0, n_chunks + 1)
    def _(c):
        for g in range(groups):
            beat = c * groups + g
            pass_on(beat)
            if g == 0:

                @pl.when(c == 2)
                def _():
                    w_copy.start()

            merge_up(beat - 3)
            if g == 0:

                @pl.when(c >= 1)
                def _():
                    attend_all(c - 1, groups - 1)

            else:

                @pl.when(c < n_chunks)
                def _():
                    attend_all(c, g - 1)

            @pl.when(c >= 2)
            def _():
                finish(c - 2, g)

    out_width = wo.shape[2]
    n_parts = max(1, out_width // 512)
    part_width = out_width // n_parts
    done = n_chunks - 1

    def all_parts():
        return [slice(p * part_width, (p + 1) * part_width) for p in range(n_parts)]

    def spread(first, last_):
        return jnp.concatenate(
            [hid_nat[c, my_rows, :] for c in range(first, last_)]
            + [hid_in[c] for c in range(first, last_)],
            axis=1,
        )

    def weights_of(first, last_, lanes):
        rows_ = slice(first * LANES, last_ * LANES)
        return jnp.concatenate([wo[0, rows_, lanes], wo[1, rows_, lanes]], axis=0)

    merge_up(n_pieces - 1)
    local[4].wait()
    w_copy.wait()
    for c in range(done):
        hidden_copy(c).wait_recv()
    sofar = spread(0, done)
    for lanes in all_parts():
        part_sum[:, lanes] = jnp.dot(
            sofar, weights_of(0, done, lanes), preferred_element_type=F32
        )
    for g in range(groups):
        finish(done, g)

    ordered = jnp.concatenate(
        [
            jnp.concatenate(
                [
                    logs[c * groups + g, i * heads_per + j : i * heads_per + j + 1, :]
                    for g in range(groups)
                    for i in range(per_group)
                ],
                axis=1,
            )
            for c in range(n_chunks)
            for j in range(heads_per)
        ],
        axis=0,
    )
    high = ordered.astype(BF16)
    left = ordered - high.astype(F32)
    middle = left.astype(BF16)
    low = (left - middle.astype(F32)).astype(BF16)
    log_sums[...] = functools.reduce(
        jnp.add,
        [
            jnp.dot(piece, back_perm[...], preferred_element_type=F32)
            for piece in (low, middle, high)
        ],
    )
    for c in range(done, n_chunks):
        hidden_copy(c).wait_recv()
    late = spread(done, n_chunks)
    for lanes in all_parts():
        rest = jnp.dot(late, weights_of(done, n_chunks, lanes), preferred_element_type=F32)
        mixed[:, lanes] = (part_sum[:, lanes] + rest).astype(BF16)

    @pl.loop(0, n_chunks)
    def _(c):
        key_copy(c, 0).wait_send()
        key_copy(c, 1).wait_send()
        value_copy(c).wait_send()
        hidden_copy(c).wait_send()

    @pl.loop(0, n_pieces)
    def _(s):
        @pl.when(has_down)
        def _():
            query_copy(s, 0).wait_send()

        @pl.when(has_down & has_up)
        def _():
            query_copy(s, 1).wait_send()

        @pl.when(has_far)
        def _():
            for copy in out_copies(FAR, s):
                copy.wait_send()

        @pl.when(has_up)
        def _():
            for copy in out_copies(UP, s):
                copy.wait_send()


def deliver(mixed, log_sums, mixed_out, log_sums_out, sems):
    copies = [
        pltpu.make_async_copy(mixed, mixed_out, sems.at[0]),
        pltpu.make_async_copy(log_sums, log_sums_out, sems.at[1]),
    ]
    for copy in copies:
        copy.start()
    for copy in copies:
        copy.wait()


def body(n_sp, tokens, w_query, w_key, w_value, w_out):
    half, depth = tokens.shape
    length = 2 * half
    width = w_query.shape[1]
    out_width = w_out.shape[1]
    heads = width // HEAD_DIM
    chunks = width // LANES
    assert REACH == MIDDLE_DILATION * length and n_sp % 2 == 0
    per = length // MIDDLE_DILATION
    groups = 2
    pieces, wide = chunks * groups, length // groups
    stats = MIDDLE_DILATION // groups * (LANES // HEAD_DIM)
    tables = (4 * MIDDLE_DILATION - 1) * per
    hbm = pl.BlockSpec(memory_space=pl.ANY)
    vmem = pl.BlockSpec(memory_space=pltpu.VMEM)
    dma = pltpu.SemaphoreType.DMA
    results = pl.pallas_call(
        functools.partial(kernel, n_sp),
        out_shape=(
            jax.ShapeDtypeStruct((half, out_width), BF16),
            jax.ShapeDtypeStruct((heads, length), F32),
        ),
        in_specs=[hbm] * 5,
        out_specs=(vmem, vmem),
        scratch_shapes=[
            pltpu.VMEM((half, depth), BF16),
            pltpu.VMEM((MIDDLE_DILATION, 2, per // 2, depth), BF16),
            pltpu.VMEM((depth, width), BF16),
            pltpu.VMEM((depth, width), BF16),
            pltpu.VMEM((depth, width), BF16),
            pltpu.VMEM((2, width, out_width), BF16),
            pltpu.VMEM((2, MIDDLE_DILATION, 2, per // 2, width), BF16),
            pltpu.VMEM((2, chunks, MIDDLE_DILATION, 2, per // 2, LANES), BF16),
            pltpu.VMEM((2, chunks, LANES, length), BF16),
            pltpu.VMEM((chunks, LANES, per), BF16),
            pltpu.VMEM((3, pieces, LANES, wide), BF16),
            pltpu.VMEM((half, half), BF16),
            pltpu.VMEM((length, length), BF16),
            pltpu.VMEM((length, per), BF16),
            pltpu.VMEM((chunks, tables, 2 * per), F32),
            pltpu.VMEM((3, pieces, stats, per), F32),
            pltpu.VMEM((3, pieces, stats, per), F32),
            pltpu.VMEM((3, pieces, LANES, wide), F32),
            pltpu.VMEM((2, pieces, LANES, wide), BF16),
            pltpu.VMEM((2, pieces, stats, per), F32),
            pltpu.VMEM((2, pieces, LANES, wide), BF16),
            pltpu.VMEM((2, pieces, stats, per), F32),
            pltpu.VMEM((chunks, LANES, length), BF16),
            pltpu.VMEM((chunks, length, LANES), BF16),
            pltpu.VMEM((pieces, stats, per), F32),
            pltpu.VMEM((chunks, half, LANES), BF16),
            pltpu.VMEM((half, out_width), F32),
            dma((5,)),
            dma,
            dma,
            dma((chunks, 3)),
            dma((chunks, 3)),
            dma((2, pieces)),
            dma((2, pieces)),
            dma((2, pieces, 2)),
            dma((2, pieces, 2)),
            dma((chunks,)),
            dma((chunks,)),
            dma,
            dma,
        ],
        compiler_params=pltpu.CompilerParams(
            collective_id=0, has_side_effects=True, vmem_limit_bytes=52 * 1024 * 1024
        ),
        name="dilated_layer",
    )(tokens, w_query, w_key, w_value, w_out)
    return pl.pallas_call(
        deliver,
        out_shape=tuple(jax.ShapeDtypeStruct(r.shape, r.dtype) for r in results),
        in_specs=[vmem, vmem],
        out_specs=(hbm, hbm),
        scratch_shapes=[dma((2,))],
        compiler_params=pltpu.CompilerParams(vmem_limit_bytes=8 * 1024 * 1024),
        name="deliver",
    )(*results)


def solution(mesh):
    in_specs = (
        P(("grp", "sp", "tp"), None),
        P(None, "tp"),
        P(None, "tp"),
        P(None, "tp"),
        P("tp", None),
    )
    out_specs = (P(("grp", "sp", "tp"), None), P("tp", ("grp", "sp")))
    return jax.shard_map(
        functools.partial(body, mesh.shape["sp"]),
        mesh=mesh,
        in_specs=in_specs,
        out_specs=out_specs,
        check_vma=False,
    )
```

```python
import functools
import math

import jax
import jax.numpy as jnp
from jax import lax
from jax.experimental import pallas as pl
from jax.experimental.pallas import tpu as pltpu
from jax.sharding import PartitionSpec as P

HEADS = 16
HEAD_DIM = 64
WINDOW_KEY_STEPS = 128
MIDDLE_DILATION = 4
FAR_DILATION = 16
REACH = 2048
ALIBI_EXP = 16.0
LANES = 128
ONES = 16
F32 = jnp.float32
BF16 = jnp.bfloat16
FAR, UP, OWN = 0, 1, 2


def log_multiplicity(distance):
    def window(stride):
        inside = (distance >= 0) & (distance <= WINDOW_KEY_STEPS * stride)
        if stride > 1:
            inside = inside & ((distance & (stride - 1)) == 0)
        return inside.astype(jnp.int32)

    count = window(1) + window(MIDDLE_DILATION) + window(FAR_DILATION)
    return jnp.where(
        count == 3,
        math.log(3.0),
        jnp.where(count == 2, math.log(2.0), jnp.where(count == 1, 0.0, -jnp.inf)),
    ).astype(F32)


def kernel(
    n_sp,
    tokens,
    w_query,
    w_key,
    w_value,
    w_out,
    mixed,
    log_sums,
    xin,
    x,
    wq,
    wk,
    wv,
    wo,
    nat,
    kbuf,
    vbuf,
    vtail,
    qbuf,
    half_perm,
    back_perm,
    tail_pick,
    tab,
    m_ref,
    l_ref,
    acc,
    o_out,
    s_out,
    o_in,
    s_in,
    hid,
    hid_nat,
    logs,
    hid_in,
    part_sum,
    local_sem,
    x_send,
    x_recv,
    kv_send,
    kv_recv,
    q_send,
    q_recv,
    o_send,
    o_recv,
    h_send,
    h_recv,
    w_send,
    w_recv,
):
    half, depth = tokens.shape
    length = 2 * half
    n_chunks = kbuf.shape[1]
    classes = MIDDLE_DILATION
    per = length // classes
    per_half = per // 2
    me = lax.axis_index("sp")
    core = lax.axis_index("tp")
    other = 1 - core
    odd = lax.rem(me, 2)
    mate = me + 1 - 2 * odd
    is_even = odd == 0
    is_odd = odd == 1
    has_up = me + 2 < n_sp
    has_far = me + 4 < n_sp
    has_down = me >= 2
    up = jnp.where(has_up, me + 2, me - 2)
    down = jnp.where(has_down, me - 2, me + 2)

    local = [
        pltpu.make_async_copy(tokens, xin, local_sem.at[0]),
        pltpu.make_async_copy(w_key, wk, local_sem.at[1]),
        pltpu.make_async_copy(w_query, wq, local_sem.at[2]),
        pltpu.make_async_copy(w_value, wv, local_sem.at[3]),
        pltpu.make_async_copy(w_out, wo.at[0], local_sem.at[4]),
    ]
    for copy in local[:4]:
        copy.start()

    barrier = pltpu.get_barrier_semaphore()
    pl.semaphore_signal(barrier, inc=1, device_id={"tp": other})
    pl.semaphore_signal(barrier, inc=1, device_id={"sp": mate})

    @pl.when(has_up)
    def _():
        pl.semaphore_signal(barrier, inc=1, device_id={"sp": me + 2})

    @pl.when(has_down)
    def _():
        pl.semaphore_signal(barrier, inc=1, device_id={"sp": me - 2})

    half_rows = lax.broadcasted_iota(jnp.int32, (half, half), 0)
    half_cols = lax.broadcasted_iota(jnp.int32, (half, half), 1)
    half_bits = per_half.bit_length() - 1
    half_time = classes * (half_rows & (per_half - 1)) + (half_rows >> half_bits)
    half_perm[...] = (half_time == half_cols).astype(F32).astype(BF16)

    local[0].wait()
    x[:, core] = (
        jnp.dot(half_perm[...], xin[...], preferred_element_type=F32)
        .astype(BF16)
        .reshape(classes, per_half, depth)
    )
    peers = 2 + jnp.where(has_up, 1, 0) + jnp.where(has_down, 1, 0)
    pl.semaphore_wait(barrier, peers)
    x_copies = [
        pltpu.make_async_remote_copy(
            src_ref=x.at[pl.ds(first, classes // 2), core],
            dst_ref=x.at[pl.ds(first, classes // 2), core],
            send_sem=x_send.at[i],
            recv_sem=x_recv.at[i],
            device_id={"tp": other},
        )
        for i, first in enumerate((0, classes // 2))
    ]
    for copy in x_copies:
        copy.start()
    my_rows = pl.ds(pl.multiple_of(core * half, half), half)
    their_rows = pl.ds(pl.multiple_of(other * half, half), half)

    def project(weights, side):
        rows = x[:, side].reshape(half, depth)
        return jnp.dot(rows, weights[...], preferred_element_type=F32)

    def place_keys(side):
        keys = project(wk, side).astype(BF16)
        for c in range(n_chunks):
            piece = keys[:, c * LANES : (c + 1) * LANES]
            kbuf[0, c, :, side] = piece.reshape(classes, per_half, LANES)

    def place_queries(side, first=0, count=classes):
        rows = x[first : first + count, side].reshape(count * per_half, depth)
        queries = jnp.dot(rows, wq[...], preferred_element_type=F32)
        queries = (queries * HEAD_DIM**-0.5).astype(BF16)
        nat[0, first : first + count, side] = queries.reshape(
            count, per_half, queries.shape[1]
        )

    def place_values(side):
        values = project(wv, side).astype(BF16)
        nat[1, :, side] = values.reshape(classes, per_half, values.shape[1])

    def key_copy(c, late):
        side = core + late * (1 - 2 * core)
        return pltpu.make_async_remote_copy(
            src_ref=kbuf.at[0, c, :, side],
            dst_ref=kbuf.at[1, c, :, side],
            send_sem=kv_send.at[c, late],
            recv_sem=kv_recv.at[c, late],
            device_id={"sp": mate},
        )

    def value_copy(c):
        return pltpu.make_async_remote_copy(
            src_ref=vbuf.at[0, c],
            dst_ref=vbuf.at[1, c],
            send_sem=kv_send.at[c, 2],
            recv_sem=kv_recv.at[c, 2],
            device_id={"sp": mate},
        )

    def query_copy(s, relay):
        return pltpu.make_async_remote_copy(
            src_ref=qbuf.at[relay, s],
            dst_ref=qbuf.at[relay + 1, s],
            send_sem=q_send.at[relay, s],
            recv_sem=q_recv.at[relay, s],
            device_id={"sp": down},
        )

    def out_copies(kind, s):
        return [
            pltpu.make_async_remote_copy(
                src_ref=src.at[kind, s],
                dst_ref=dst.at[kind, s],
                send_sem=o_send.at[kind, s, i],
                recv_sem=o_recv.at[kind, s, i],
                device_id={"sp": up},
            )
            for i, (src, dst) in enumerate(((o_out, o_in), (s_out, s_in)))
        ]

    def hidden_copy(c):
        return pltpu.make_async_remote_copy(
            src_ref=hid_nat.at[c, their_rows],
            dst_ref=hid_in.at[c],
            send_sem=h_send.at[c],
            recv_sem=h_recv.at[c],
            device_id={"tp": other},
        )

    w_copy = pltpu.make_async_remote_copy(
        src_ref=w_out,
        dst_ref=wo.at[1],
        send_sem=w_send,
        recv_sem=w_recv,
        device_id={"tp": other},
    )

    def turned(which, c):
        lanes = slice(c * LANES, (c + 1) * LANES)
        return nat[which].reshape(length, n_chunks * LANES)[:, lanes].T

    local[1].wait()
    place_keys(core)
    early = n_chunks // 2
    for c in range(early):
        key_copy(c, 0).start()
    local[2].wait()
    place_queries(core)
    local[3].wait()
    local[4].start()
    place_values(core)

    groups = 2
    wide = length // groups
    per_group = classes // groups
    for g in range(groups):
        x_copies[g].wait()
        place_queries(other, g * per_group, per_group)
        for c in range(n_chunks):
            lanes = slice(c * LANES, (c + 1) * LANES)
            rows = nat[0, g * per_group : (g + 1) * per_group, :, :, lanes]
            qbuf[0, c * groups + g] = rows.reshape(wide, LANES).T
            if c == 0:

                @pl.when(has_down)
                def _():
                    query_copy(g, 0).start()

    place_keys(other)
    key_copy(0, 1).start()
    place_values(other)
    for c in range(n_chunks):
        if c >= early:
            key_copy(c, 0).start()
        if c >= 1:
            key_copy(c, 1).start()
        vbuf[0, c] = turned(1, c)
        value_copy(c).start()

    key_step = lax.broadcasted_iota(jnp.int32, (per, per), 0)
    query_step = lax.broadcasted_iota(jnp.int32, (per, per), 1)
    tail = per // classes
    tail_bits = tail.bit_length() - 1
    heads_per = LANES // HEAD_DIM

    def slope_of(head):
        number = core * (n_chunks * heads_per) + head + 1
        exponent = jnp.full((1, per), number, jnp.int32).astype(F32)
        return jnp.exp2(exponent * (-ALIBI_EXP / HEADS))

    slopes = [slope_of(h) for h in range(n_chunks * heads_per)]

    def fill(first_row, distance, logc):
        gap = distance.astype(F32)
        rows = pl.ds(pl.multiple_of(first_row, per), per)
        for h in range(n_chunks * heads_per):
            c, j = divmod(h, heads_per)
            tab[c, rows, j * per : (j + 1) * per] = logc - slopes[h] * gap

    steps = classes * (query_step - key_step)
    T0 = 0
    T_CLASS = (2 * classes - 1) * per
    T_TAIL = T_CLASS + classes * per

    @pl.loop(0, 2 * classes - 1)
    def _(e):
        distance = steps + (classes - 1 - e)
        fill(T0 + e * per, distance, log_multiplicity(distance))

    @pl.loop(0, classes)
    def _(e):
        distance = steps + (e + 1) * length
        fill(T_CLASS + e * per, distance, log_multiplicity(distance))

    tail_class = key_step >> tail_bits
    tail_step = (key_step & (tail - 1)) + (per - tail)

    @pl.loop(0, classes)
    def _(r):
        distance = length + classes * (query_step - tail_step) + (r - tail_class)
        logc = jnp.where(tail_class == r, -jnp.inf, log_multiplicity(distance))
        fill(T_TAIL + r * per, distance, logc)

    rows = lax.broadcasted_iota(jnp.int32, (length, length), 0)
    cols = lax.broadcasted_iota(jnp.int32, (length, length), 1)
    per_bits = per.bit_length() - 1
    time_of_row = classes * (rows & (per - 1)) + (rows >> per_bits)
    back_perm[...] = (time_of_row == cols).astype(F32).astype(BF16)
    pick_rows = lax.broadcasted_iota(jnp.int32, (length, per), 0)
    pick_cols = lax.broadcasted_iota(jnp.int32, (length, per), 1)
    pick = (pick_cols >> tail_bits) * per + (per - tail) + (pick_cols & (tail - 1))
    tail_pick[...] = (pick_rows == pick).astype(F32).astype(BF16)

    ones_of = functools.partial(jnp.ones, dtype=BF16)

    def class_part(slot, c, r, table):
        keys = kbuf[slot, c, r].reshape(per, LANES)
        bias = tab[c, table : table + per, :]
        return keys, bias, vbuf[slot, c, :, r * per : (r + 1) * per]

    def gap_table(blocks):
        return T_CLASS + (blocks - 1) * per

    def tail_part(c, r):
        keys = jnp.concatenate(
            [kbuf[1, c, k, 1, per_half - tail :, :] for k in range(classes)], axis=0
        )
        table = T_TAIL + r * per
        return keys, tab[c, table : table + per, :], vtail[c]

    def own_part(c, r):
        first = T0 + (classes - 1 - r) * per
        return (
            kbuf[0, c].reshape(length, LANES),
            tab[c, first : first + length, :],
            vbuf[0, c],
        )

    def score(c, g, i, q_slot, parts_of):
        piece = c * groups + g
        lanes = slice(i * per, (i + 1) * per)
        parts = parts_of(g * per_group + i)
        first = qbuf[q_slot, piece, :HEAD_DIM, lanes]
        second = qbuf[q_slot, piece, HEAD_DIM:, lanes]
        blank = jnp.zeros_like(first)
        queries = jnp.concatenate(
            [
                jnp.concatenate([first, blank], axis=0),
                jnp.concatenate([blank, second], axis=0),
            ],
            axis=1,
        )
        scores = [
            jnp.dot(keys, queries, preferred_element_type=F32) + bias
            for keys, bias, _ in parts
        ]
        tops = [jnp.max(s, axis=0, keepdims=True) for s in scores]
        values = jnp.concatenate([v for _, _, v in parts], axis=1)
        return scores, functools.reduce(jnp.maximum, tops), values

    def weigh(item, c, g, i, scores, top, values):
        piece = c * groups + g
        lanes = slice(i * per, (i + 1) * per)
        weights = jnp.concatenate(
            [jnp.exp(s - top).astype(BF16) for s in scores], axis=0
        )
        count = values.shape[1]
        for j in range(heads_per):
            mine = values[j * HEAD_DIM : (j + 1) * HEAD_DIM]
            summed = jnp.dot(
                jnp.concatenate([mine, ones_of((ONES, count))], axis=0),
                weights[:, j * per : (j + 1) * per],
                preferred_element_type=F32,
            )
            row = slice(i * heads_per + j, i * heads_per + j + 1)
            acc[item, piece, j * HEAD_DIM : (j + 1) * HEAD_DIM, lanes] = summed[:HEAD_DIM]
            l_ref[item, piece, row, :] = summed[HEAD_DIM : HEAD_DIM + 1]
            m_ref[item, piece, row, :] = top[:, j * per : (j + 1) * per]

    def attend(c, g, items):
        held = None
        for i in range(per_group):
            for item, q_slot, parts_of in items:
                scored = (item, c, g, i, *score(c, g, i, q_slot, parts_of))
                if held is not None:
                    weigh(*held)
                held = scored
        weigh(*held)

    def blocks():
        for i in range(per_group):
            for j in range(heads_per):
                row = slice(i * heads_per + j, i * heads_per + j + 1)
                dims = slice(j * HEAD_DIM, (j + 1) * HEAD_DIM)
                yield row, dims, slice(i * per, (i + 1) * per)

    def take_in(item, s, kind):
        for copy in out_copies(kind, s):
            copy.wait_recv()
        here, there = m_ref[item, s], s_in[kind, s]
        top = jnp.maximum(here, there)
        keep, gain = jnp.exp(here - top), jnp.exp(there - top)
        m_ref[item, s] = top
        l_ref[item, s] = keep * l_ref[item, s] + gain
        for row, dims, lanes in blocks():
            acc[item, s, dims, lanes] = (
                keep[row] * acc[item, s, dims, lanes]
                + gain[row] * o_in[kind, s, dims, lanes].astype(F32)
            )

    def level(item, s, out):
        total = l_ref[item, s]
        scale = 1.0 / total
        for row, dims, lanes in blocks():
            out[dims, lanes] = (acc[item, s, dims, lanes] * scale[row]).astype(BF16)
        return m_ref[item, s] + jnp.log(total)

    def emit(item, s):
        s_out[item, s] = level(item, s, o_out.at[item, s])
        for copy in out_copies(item, s):
            copy.start()

    def finish(c, g):
        piece = c * groups + g

        @pl.when(has_down)
        def _():
            take_in(OWN, piece, UP)

        logs[piece] = level(OWN, piece, hid.at[c, :, g * wide : (g + 1) * wide])
        if g == groups - 1:
            hid_nat[c] = (
                jnp.dot(hid[c], back_perm[...], preferred_element_type=F32).astype(BF16).T
            )
            hidden_copy(c).start()

    n_pieces = n_chunks * groups

    def merge_up(s):
        @pl.when(has_up & (s >= 0) & (s < n_pieces))
        def _():
            @pl.when(has_down)
            def _():
                take_in(UP, s, FAR)

            emit(UP, s)

    def pass_on(s):
        @pl.when(has_up & (s < n_pieces))
        def _():
            query_copy(s, 0).wait_recv()

            @pl.when(has_down)
            def _():
                query_copy(s, 1).start()

        @pl.when(has_down & (s + groups < n_pieces))
        def _():
            query_copy(s + groups, 0).start()

    def attend_all(c, g):
        if g == 0:
            key_copy(c, 0).wait_recv()
            key_copy(c, 1).wait_recv()
            value_copy(c).wait_recv()
            vtail[c] = jnp.dot(
                vbuf[1, c], tail_pick[...], preferred_element_type=F32
            ).astype(BF16)

        piece = c * groups + g

        @pl.when(has_far)
        def _():
            query_copy(piece, 1).wait_recv()

            @pl.when(is_even)
            def _():
                attend(
                    c,
                    g,
                    [
                        (
                            FAR,
                            2,
                            lambda r: [
                                class_part(0, c, r, gap_table(4)),
                                class_part(1, c, r, gap_table(3)),
                            ],
                        ),
                    ],
                )

            @pl.when(is_odd)
            def _():
                attend(c, g, [(FAR, 2, lambda r: [class_part(0, c, r, gap_table(4))])])

            emit(FAR, piece)

        @pl.when(is_even)
        def _():
            attend(
                c,
                g,
                [
                    (
                        UP,
                        1,
                        lambda r: [
                            class_part(0, c, r, gap_table(2)),
                            class_part(1, c, r, gap_table(1)),
                            tail_part(c, r),
                        ],
                    ),
                    (OWN, 0, lambda r: [own_part(c, r)]),
                ],
            )

        @pl.when(is_odd)
        def _():
            attend(
                c,
                g,
                [
                    (
                        UP,
                        1,
                        lambda r: [
                            class_part(0, c, r, gap_table(2)),
                            class_part(1, c, r, gap_table(3)),
                        ],
                    ),
                    (
                        OWN,
                        0,
                        lambda r: [
                            own_part(c, r),
                            class_part(1, c, r, gap_table(1)),
                            tail_part(c, r),
                        ],
                    ),
                ],
            )

    @pl.loop(0, n_chunks + 1)
    def _(c):
        for g in range(groups):
            beat = c * groups + g
            pass_on(beat)
            if g == 0:

                @pl.when(c == 2)
                def _():
                    w_copy.start()

            merge_up(beat - 3)
            if g == 0:

                @pl.when(c >= 1)
                def _():
                    attend_all(c - 1, groups - 1)

            else:

                @pl.when(c < n_chunks)
                def _():
                    attend_all(c, g - 1)

            @pl.when(c >= 2)
            def _():
                finish(c - 2, g)

    out_width = wo.shape[2]
    n_parts = max(1, out_width // 512)
    part_width = out_width // n_parts
    done = n_chunks - 1

    def all_parts():
        return [slice(p * part_width, (p + 1) * part_width) for p in range(n_parts)]

    def spread(first, last_):
        return jnp.concatenate(
            [hid_nat[c, my_rows, :] for c in range(first, last_)]
            + [hid_in[c] for c in range(first, last_)],
            axis=1,
        )

    def weights_of(first, last_, lanes):
        rows_ = slice(first * LANES, last_ * LANES)
        return jnp.concatenate([wo[0, rows_, lanes], wo[1, rows_, lanes]], axis=0)

    merge_up(n_pieces - 1)
    local[4].wait()
    w_copy.wait()
    for c in range(done):
        hidden_copy(c).wait_recv()
    sofar = spread(0, done)
    for lanes in all_parts():
        part_sum[:, lanes] = jnp.dot(
            sofar, weights_of(0, done, lanes), preferred_element_type=F32
        )
    for g in range(groups):
        finish(done, g)

    ordered = jnp.concatenate(
        [
            jnp.concatenate(
                [
                    logs[c * groups + g, i * heads_per + j : i * heads_per + j + 1, :]
                    for g in range(groups)
                    for i in range(per_group)
                ],
                axis=1,
            )
            for c in range(n_chunks)
            for j in range(heads_per)
        ],
        axis=0,
    )
    high = ordered.astype(BF16)
    left = ordered - high.astype(F32)
    middle = left.astype(BF16)
    low = (left - middle.astype(F32)).astype(BF16)
    log_sums[...] = functools.reduce(
        jnp.add,
        [
            jnp.dot(piece, back_perm[...], preferred_element_type=F32)
            for piece in (low, middle, high)
        ],
    )
    for c in range(done, n_chunks):
        hidden_copy(c).wait_recv()
    late = spread(done, n_chunks)
    for lanes in all_parts():
        rest = jnp.dot(late, weights_of(done, n_chunks, lanes), preferred_element_type=F32)
        mixed[:, lanes] = (part_sum[:, lanes] + rest).astype(BF16)

    @pl.loop(0, n_chunks)
    def _(c):
        key_copy(c, 0).wait_send()
        key_copy(c, 1).wait_send()
        value_copy(c).wait_send()
        hidden_copy(c).wait_send()

    @pl.loop(0, n_pieces)
    def _(s):
        @pl.when(has_down)
        def _():
            query_copy(s, 0).wait_send()

        @pl.when(has_down & has_up)
        def _():
            query_copy(s, 1).wait_send()

        @pl.when(has_far)
        def _():
            for copy in out_copies(FAR, s):
                copy.wait_send()

        @pl.when(has_up)
        def _():
            for copy in out_copies(UP, s):
                copy.wait_send()


def deliver(mixed, log_sums, mixed_out, log_sums_out, sems):
    copies = [
        pltpu.make_async_copy(mixed, mixed_out, sems.at[0]),
        pltpu.make_async_copy(log_sums, log_sums_out, sems.at[1]),
    ]
    for copy in copies:
        copy.start()
    for copy in copies:
        copy.wait()


def body(n_sp, tokens, w_query, w_key, w_value, w_out):
    half, depth = tokens.shape
    length = 2 * half
    width = w_query.shape[1]
    out_width = w_out.shape[1]
    heads = width // HEAD_DIM
    chunks = width // LANES
    assert REACH == MIDDLE_DILATION * length and n_sp % 2 == 0
    per = length // MIDDLE_DILATION
    groups = 2
    pieces, wide = chunks * groups, length // groups
    stats = MIDDLE_DILATION // groups * (LANES // HEAD_DIM)
    tables = (4 * MIDDLE_DILATION - 1) * per
    hbm = pl.BlockSpec(memory_space=pl.ANY)
    vmem = pl.BlockSpec(memory_space=pltpu.VMEM)
    dma = pltpu.SemaphoreType.DMA
    results = pl.pallas_call(
        functools.partial(kernel, n_sp),
        out_shape=(
            jax.ShapeDtypeStruct((half, out_width), BF16),
            jax.ShapeDtypeStruct((heads, length), F32),
        ),
        in_specs=[hbm] * 5,
        out_specs=(vmem, vmem),
        scratch_shapes=[
            pltpu.VMEM((half, depth), BF16),
            pltpu.VMEM((MIDDLE_DILATION, 2, per // 2, depth), BF16),
            pltpu.VMEM((depth, width), BF16),
            pltpu.VMEM((depth, width), BF16),
            pltpu.VMEM((depth, width), BF16),
            pltpu.VMEM((2, width, out_width), BF16),
            pltpu.VMEM((2, MIDDLE_DILATION, 2, per // 2, width), BF16),
            pltpu.VMEM((2, chunks, MIDDLE_DILATION, 2, per // 2, LANES), BF16),
            pltpu.VMEM((2, chunks, LANES, length), BF16),
            pltpu.VMEM((chunks, LANES, per), BF16),
            pltpu.VMEM((3, pieces, LANES, wide), BF16),
            pltpu.VMEM((half, half), BF16),
            pltpu.VMEM((length, length), BF16),
            pltpu.VMEM((length, per), BF16),
            pltpu.VMEM((chunks, tables, 2 * per), F32),
            pltpu.VMEM((3, pieces, stats, per), F32),
            pltpu.VMEM((3, pieces, stats, per), F32),
            pltpu.VMEM((3, pieces, LANES, wide), F32),
            pltpu.VMEM((2, pieces, LANES, wide), BF16),
            pltpu.VMEM((2, pieces, stats, per), F32),
            pltpu.VMEM((2, pieces, LANES, wide), BF16),
            pltpu.VMEM((2, pieces, stats, per), F32),
            pltpu.VMEM((chunks, LANES, length), BF16),
            pltpu.VMEM((chunks, length, LANES), BF16),
            pltpu.VMEM((pieces, stats, per), F32),
            pltpu.VMEM((chunks, half, LANES), BF16),
            pltpu.VMEM((half, out_width), F32),
            dma((5,)),
            dma((2,)),
            dma((2,)),
            dma((chunks, 3)),
            dma((chunks, 3)),
            dma((2, pieces)),
            dma((2, pieces)),
            dma((2, pieces, 2)),
            dma((2, pieces, 2)),
            dma((chunks,)),
            dma((chunks,)),
            dma,
            dma,
        ],
        compiler_params=pltpu.CompilerParams(
            collective_id=0, has_side_effects=True, vmem_limit_bytes=52 * 1024 * 1024
        ),
        name="dilated_layer",
    )(tokens, w_query, w_key, w_value, w_out)
    return pl.pallas_call(
        deliver,
        out_shape=tuple(jax.ShapeDtypeStruct(r.shape, r.dtype) for r in results),
        in_specs=[vmem, vmem],
        out_specs=(hbm, hbm),
        scratch_shapes=[dma((2,))],
        compiler_params=pltpu.CompilerParams(vmem_limit_bytes=8 * 1024 * 1024),
        name="deliver",
    )(*results)


def solution(mesh):
    in_specs = (
        P(("grp", "sp", "tp"), None),
        P(None, "tp"),
        P(None, "tp"),
        P(None, "tp"),
        P("tp", None),
    )
    out_specs = (P(("grp", "sp", "tp"), None), P("tp", ("grp", "sp")))
    return jax.shard_map(
        functools.partial(body, mesh.shape["sp"]),
        mesh=mesh,
        in_specs=in_specs,
        out_specs=out_specs,
        check_vma=False,
    )
```
